32 devices in a mesh: fs: 8 (over z, y), tp: 4 (over x, core).
Axes of the slice: x: 2, y: 2, z: 4, core: 2. Of those that a mesh axis runs over, the one named last changes fastest.
Arguments:
- hidden_in: bfloat16 [512, 4096], P(None, 'tp'), may hold values from -6 to 6
- up_act: bfloat16 [512, 12288], P('tp', 'fs'), may hold values from -6 to 6
- up_val: bfloat16 [512, 12288], P('tp', 'fs'), may hold values from -6 to 6
- cotangent: bfloat16 [512, 4096], P('tp'), may hold values from -6 to 6
- w_act: bfloat16 [4096, 12288], P('tp', 'fs'), may hold values from -0.09375 to 0.09375
- w_val: bfloat16 [4096, 12288], P('tp', 'fs'), may hold values from -0.09375 to 0.09375
- w_down: bfloat16 [12288, 4096], P('fs', 'tp'), may hold values from -0.0546875 to 0.0546875
- conv_act: bfloat16 [3, 12288], P(None, 'fs'), may hold values from -3 to 3
- conv_val: bfloat16 [3, 12288], P(None, 'fs'), may hold values from -3 to 3
- bias_act: bfloat16 [12288], P('fs'), may hold values from -3 to 3
- bias_val: bfloat16 [12288], P('fs'), may hold values from -3 to 3
Outputs:
- grad_input: bfloat16 [512, 4096], P(('tp', 'fs'))
- grad_w_act: float32 [4096, 12288], P('tp', 'fs')
- grad_w_val: float32 [4096, 12288], P('tp', 'fs')
- grad_w_down: float32 [12288, 4096], P('fs', 'tp')
- grad_conv_act: float32 [3, 12288], P(None, 'fs')
- grad_conv_val: float32 [3, 12288], P(None, 'fs')
- grad_bias_act: float32 [12288], P('fs')
- grad_bias_val: float32 [12288], P('fs')
- rows_act: float32 [4096], P('tp')
- rows_val: float32 [4096], P('tp')
- rows_down: float32 [12288], P('fs')
- conv_rows: float32 [2, 3], replicated
The draws below stay inside these ranges and needn't reach their ends.
All inputs are finite; a program needn't handle non-finite values.
Results may differ from the reference program's by a relative error of at most 0.0057.
Values may be sent and summed in bfloat16 or wider, within the bound.
A program may use at most 128 MiB of HBM per device.

```python
import jax
import jax.numpy as jnp
from jax import lax

D = 4096
FF = 12288
KW = 3
TOKENS = 512


def with_spikes(result, own_key, source, target, parts, factor):
    owner, partner = [(jnp.arange(result.shape[axis_at]) // (result.shape[axis_at] // parts)).reshape([-1 if axis == axis_at else 1 for axis in range(result.ndim)]) for axis_at in (source, target)]
    chosen = jax.random.permutation(own_key, parts)[partner]
    strong = (owner == chosen) | (owner == (partner + parts // 2) % parts)
    return jnp.where(strong, factor * result, result)


def shard_levels(own_key, shape, cuts, smallest, top_value):
    level = 1.0
    for axis_at, parts in cuts:
        draws = jax.random.uniform(jax.random.fold_in(jax.random.fold_in(own_key, 6), axis_at), (parts,), jnp.float32, smallest / len(cuts), top_value / len(cuts))
        level = level * jnp.repeat(jnp.exp(draws), shape[axis_at] // parts).reshape((-1,) + (1,) * (len(shape) - 1 - axis_at))
    return level


def bell_draw(own_key, extent, deviation, bound, pieces=(), held_as=jnp.bfloat16):
    values = deviation * jax.random.normal(own_key, extent, jnp.float32)
    if pieces:
        values = values * shard_levels(own_key, extent, pieces, -0.22, 0.18)
    return jnp.clip(values, -bound, bound).astype(held_as)


def noise_with(own_key, dims, scale, most, cuts, heavy, dtype=jnp.bfloat16):
    entries = scale * jax.random.normal(own_key, dims, jnp.float32)
    if cuts:
        entries = entries * shard_levels(own_key, dims, cuts, -0.22, 0.18)
    return jnp.clip(with_spikes(entries, jax.random.fold_in(own_key, 3), *heavy), -most, most).astype(dtype)


def setup_inputs(seed: int = 0) -> dict:
    key_of = jax.random.split(jax.random.key(seed), 12)
    return {
        "hidden_in": bell_draw(key_of[0], (TOKENS, D), 1.0, 6.0, ((1, 4),)),
        "up_act": bell_draw(key_of[1], (TOKENS, FF), 1.0, 6.0, ((0, 4), (1, 8))),
        "up_val": bell_draw(key_of[2], (TOKENS, FF), 1.0, 6.0, ((0, 4), (1, 8))),
        "cotangent": noise_with(key_of[3], (TOKENS, D), 1.0, 6.0, ((0, 4),), (0, 1, 4, 2.0)),
        "w_act": bell_draw(key_of[4], (D, FF), D ** -0.5, 0.09375, ((0, 4), (1, 8))),
        "w_val": bell_draw(key_of[5], (D, FF), D ** -0.5, 0.09375, ((0, 4), (1, 8))),
        "w_down": bell_draw(key_of[6], (FF, D), FF ** -0.5, 0.0546875, ((0, 8), (1, 4))),
        "conv_act": bell_draw(key_of[7], (KW, FF), 0.577, 3.0, ((1, 8),)),
        "conv_val": bell_draw(key_of[8], (KW, FF), 0.577, 3.0, ((1, 8),)),
        "bias_act": bell_draw(key_of[9], (FF,), 0.5, 3.0, ((0, 8),)),
        "bias_val": bell_draw(key_of[10], (FF,), 0.5, 3.0, ((0, 8),)),
    }


def conv_ahead(upper, taps, bias):
    length = upper.shape[0]
    padded = jnp.concatenate([jnp.zeros((KW - 1, upper.shape[1]), jnp.float32), upper.astype(jnp.float32)], 0)
    total = jnp.zeros(upper.shape, jnp.float32) + bias.astype(jnp.float32)
    for offset in range(KW):
        total = total + taps[offset].astype(jnp.float32) * padded[offset:offset + length]
    return (total, padded)

def conv_behind(grad_pre, taps):
    length = grad_pre.shape[0]
    padded = jnp.concatenate([grad_pre, jnp.zeros((KW - 1, grad_pre.shape[1]), jnp.float32)], 0)
    total = jnp.zeros(grad_pre.shape, jnp.float32)
    for offset in range(KW):
        total = total + taps[offset].astype(jnp.float32) * padded[KW - 1 - offset:KW - 1 - offset + length]
    return total.astype(jnp.bfloat16)

def tap_grads(grad_pre, padded):
    length = grad_pre.shape[0]
    rows = [lax.optimization_barrier(jnp.sum(grad_pre * padded[offset:offset + length], axis=0)) for offset in range(KW)]
    return (jnp.stack(rows, 0), lax.optimization_barrier(jnp.sum(grad_pre, axis=0)))

def reference(hidden_in, up_act, up_val, cotangent, w_act, w_val, w_down, conv_act, conv_val, bias_act, bias_val):
    pre_act, padded_act = conv_ahead(up_act, conv_act, bias_act)
    pre_val, padded_val = conv_ahead(up_val, conv_val, bias_val)
    gelu_act, gelu_back = jax.vjp(jax.nn.gelu, pre_act)
    mixed = (gelu_act * pre_val).astype(jnp.bfloat16)
    grad_mixed = jnp.dot(cotangent, w_down.T, preferred_element_type=jnp.float32).astype(jnp.bfloat16)
    grad_mixed = lax.optimization_barrier(grad_mixed).astype(jnp.float32)
    grad_pre_act = gelu_back(grad_mixed * pre_val)[0]
    grad_pre_val = grad_mixed * gelu_act
    grad_up_act = conv_behind(grad_pre_act, conv_act)
    grad_up_val = conv_behind(grad_pre_val, conv_val)
    grad_conv_act, grad_bias_act = tap_grads(grad_pre_act, padded_act)
    grad_conv_val, grad_bias_val = tap_grads(grad_pre_val, padded_val)
    grad_w_act = jnp.dot(hidden_in.T, grad_up_act, preferred_element_type=jnp.float32)
    grad_w_val = jnp.dot(hidden_in.T, grad_up_val, preferred_element_type=jnp.float32)
    grad_w_down = jnp.dot(mixed.T, cotangent, preferred_element_type=jnp.float32)
    grad_input = jnp.dot(grad_up_act, w_act.T, preferred_element_type=jnp.float32)
    grad_input = grad_input + jnp.dot(grad_up_val, w_val.T, preferred_element_type=jnp.float32)
    grad_input = grad_input.astype(jnp.bfloat16)
    rows_act = lax.optimization_barrier(jnp.sum(grad_w_act * grad_w_act, axis=1))
    rows_val = lax.optimization_barrier(jnp.sum(grad_w_val * grad_w_val, axis=1))
    rows_down = lax.optimization_barrier(jnp.sum(grad_w_down * grad_w_down, axis=1))
    conv_rows = jnp.stack([lax.optimization_barrier(jnp.sum(grad_conv_act * grad_conv_act, axis=1)), lax.optimization_barrier(jnp.sum(grad_conv_val * grad_conv_val, axis=1))], 0)
    return (grad_input, grad_w_act, grad_w_val, grad_w_down, grad_conv_act, grad_conv_val, grad_bias_act, grad_bias_val, rows_act, rows_val, rows_down, conv_rows)
```

```python
import itertools

import jax
import jax.numpy as jnp
from jax import lax
from jax.experimental import pallas as pl
from jax.experimental.pallas import tpu as pltpu
from jax.sharding import PartitionSpec as P

MESH = pl.DeviceIdType.MESH
F32 = jnp.float32
BF16 = jnp.bfloat16
CHUNK = 256
GROUP = 512
HALO = 16
TAIL = 8
COPIES = 112
ROOT_TWO_OVER_PI = 0.7978845608028654
CUBIC = 0.044715


def span(index, size):
    return pl.ds(pl.multiple_of(index * size, size), size)


def gradient_kernel(
    hidden_hbm, up_a_hbm, up_v_hbm, cot_hbm, w_a_hbm, w_v_hbm, down_hbm, params,
    columns, all_g, all_m, sums, out, norms, down_norms, squares,
    hidden, up, cot, weights, down,
    before, after, grads, gated, factor,
    own, to_sib, from_sib, to_sib_far, from_sib_far, to_far, from_far,
    terms, to_pair, from_pair, kept, to_line, from_line, settled,
    own_sums, sib_sums, chip_sums, far_sums, own_norms, got_norms, own_down, got_down,
    own_squares, got_squares,
    send, receive, loaded,
):
    me, fs = lax.axis_index("tp"), lax.axis_index("fs")
    count, fs_count = lax.axis_size("tp"), lax.axis_size("fs")
    chip, core = me // 2, me % 2
    other = 1 - chip
    sib, far, diag = chip * 2 + (1 - core), other * 2 + core, other * 2 + (1 - core)
    line = fs_count // 2
    z, y = fs // 2, fs % 2
    pair = z * 2 + (1 - y)
    z_mate = z + 1 - 2 * (z % 2)
    length, width = up.shape[1:]
    depth = down.shape[1]
    tap_count = params.shape[0] // 2 - 1
    reach = tap_count - 1
    group_count = width // GROUP
    shard = out.shape[0]
    quarter = length // 4

    def to(index):
        return {"tp": index}

    def to_fs(index):
        return {"fs": index}

    fs_others = [lax.rem(fs + by, fs_count) for by in range(1, fs_count)]
    numbers = itertools.count()
    pending = []

    def copy_of(source, target, where, send_at=None, receive_at=None):
        number = next(numbers) if send_at is None else send_at
        assert number < COPIES
        return pltpu.make_async_remote_copy(
            src_ref=source,
            dst_ref=target,
            send_sem=send.at[number],
            recv_sem=receive.at[number if receive_at is None else receive_at],
            device_id=where,
            device_id_type=MESH,
        )

    def launch(source, target, where):
        copy = copy_of(source, target, where)
        copy.start()
        pending.append(copy)
        return copy

    def rows(index):
        return span(index, length)

    def cols(index):
        return span(index, depth)

    def group(g):
        return pl.ds(g * GROUP, GROUP)

    def chunks(g, step):
        def at(i, carry):
            step(pl.ds(pl.multiple_of(g * GROUP + i * CHUNK, CHUNK), CHUNK))
            return carry

        lax.fori_loop(0, GROUP // CHUNK, at, 0)

    def depth_chunks(step):
        def at(i, carry):
            step(span(i, CHUNK))
            return carry

        lax.fori_loop(0, depth // CHUNK, at, 0)

    sources = (
        (up_a_hbm, up.at[0]), (up_v_hbm, up.at[1]), (cot_hbm, cot), (down_hbm, down),
        (hidden_hbm, hidden), (w_a_hbm, weights.at[0]), (w_v_hbm, weights.at[1]),
    )
    loads = [
        pltpu.make_async_copy(source, target, loaded.at[i])
        for i, (source, target) in enumerate(sources)
    ]
    for load in loads:
        load.start()

    barrier = pltpu.get_barrier_semaphore()
    everyone = [to(sib), to(far), to(diag)] + [to_fs(index) for index in fs_others]
    for where in everyone:
        pl.semaphore_signal(barrier, inc=1, device_id=where, device_id_type=MESH)
    pl.semaphore_wait(barrier, len(everyone))

    loads[0].wait()
    loads[1].wait()
    has_before, has_after = me > 0, me < count - 1
    last = pl.ds(length - HALO, HALO)
    halo = [copy_of(up.at[r, last, :], before.at[r], to(lax.rem(me + 1, count))) for r in range(2)]

    @pl.when(has_after)
    def _():
        for copy in halo:
            copy.start()

    @pl.when(jnp.logical_not(has_before))
    def _():
        before[...] = jnp.zeros(before.shape, before.dtype)

    @pl.when(jnp.logical_not(has_after))
    def _():
        after[...] = jnp.zeros(after.shape, after.dtype)

    loads[2].wait()
    mine = span((z % 2) * 2 + y, quarter)

    def quarter_of(index):
        at = index * length + ((z % 2) * 2 + y) * quarter
        return columns.at[pl.ds(pl.multiple_of(at, quarter), quarter), :]

    cot_far = launch(cot.at[mine, cols(far)], quarter_of(me), to(far))
    cot_diag = launch(cot.at[mine, cols(diag)], quarter_of(me), to(diag))
    cot_sib = launch(cot.at[:, cols(sib)], columns.at[rows(me), :], to(sib))
    columns[rows(me), :] = cot[:, cols(me)]

    def share(index):
        mates = (pair, z_mate * 2 + y, z_mate * 2 + (1 - y))
        return [launch(quarter_of(index), quarter_of(index), to_fs(mate)) for mate in mates]

    def shifted(r, lanes):
        ext = jnp.concatenate([before[r, :, lanes].astype(F32), up[r, :, lanes].astype(F32)], 0)
        return [ext[HALO - reach + k : HALO - reach + k + length] for k in range(tap_count)]

    def param(r, k, lanes):
        at = r * (tap_count + 1) + k
        return params[at : at + 1, lanes]

    def forward(lanes):
        pre = []
        for r in range(2):
            taken = shifted(r, lanes)
            total = jnp.broadcast_to(param(r, tap_count, lanes), (length, CHUNK))
            for k in range(tap_count):
                total = total + param(r, k, lanes) * taken[k]
            pre.append(total)
        pre_a, pre_v = pre
        square = pre_a * pre_a
        bent = jnp.tanh(ROOT_TWO_OVER_PI * pre_a * (1.0 + CUBIC * square))
        half = 0.5 * (1.0 + bent)
        gelu = pre_a * half
        slope = half + 0.5 * pre_a * (1.0 - bent * bent) * (
            ROOT_TWO_OVER_PI * (1.0 + 3.0 * CUBIC * square)
        )
        all_m[rows(me), lanes] = (gelu * pre_v).astype(BF16)
        gated[:, lanes] = gelu
        factor[:, lanes] = pre_v * slope

    mixed_far, mixed_sib = [], []

    def spread_mixed(g):
        here = all_m.at[rows(me), group(g)]
        mixed_far.append(launch(here, here, to(far)))
        mixed_sib.append(launch(here, here, to(sib)))

    @pl.when(has_before)
    def _():
        for copy in halo:
            copy.wait_recv()

    shares = []
    for g in range(group_count):
        chunks(g, forward)
        spread_mixed(g)
        if g == 0:
            cot_far.wait_recv()
            shares += share(far)
        if g == 1:
            cot_diag.wait_recv()
            shares += share(diag)

    loads[3].wait()

    def partial(index, g, finish):
        def step(lanes):
            finish(lanes, contract_last(columns[rows(index), :], down[lanes, :]))

        chunks(g, step)

    def keep(target):
        def finish(lanes, value):
            target[:, lanes] = value.astype(target.dtype)

        return finish

    def add_far(lanes, value):
        to_far[:, lanes] = (value + from_sib_far[:, lanes].astype(F32)).astype(BF16)

    for g in range(group_count):
        partial(me, g, keep(own))
    cot_sib.wait_recv()
    for g in range(group_count):
        partial(sib, g, keep(to_sib))
    near = launch(to_sib, from_sib, to(sib))
    for copy in shares:
        copy.wait_recv()

    relayed, crossed = [], []

    def diag_part(g):
        partial(diag, g, keep(to_sib_far))
        relayed.append(launch(to_sib_far.at[:, group(g)], from_sib_far.at[:, group(g)], to(sib)))

    def far_part(g):
        relayed[g].wait_recv()
        partial(far, g, add_far)
        crossed.append(launch(to_far.at[:, group(g)], from_far.at[:, group(g)], to(far)))

    diag_part(0)
    for g in range(1, group_count):
        diag_part(g)
        far_part(g - 1)
    far_part(group_count - 1)

    mixed_relays = []

    def relay_mixed(g):
        mixed_far[g].wait_recv()
        there = all_m.at[rows(far), group(g)]
        mixed_relays.append(launch(there, there, to(sib)))

    def combine(lanes):
        total = own[:, lanes] + from_sib[:, lanes].astype(F32) + from_far[:, lanes].astype(F32)
        grad_mixed = total.astype(BF16).astype(F32)
        for r, scale in ((0, factor), (1, gated)):
            pre_grad = grad_mixed * scale[:, lanes]
            grads[r, :, lanes] = pre_grad
            found = [
                jnp.sum(pre_grad * taken, axis=0, keepdims=True) for taken in shifted(r, lanes)
            ]
            found.append(jnp.sum(pre_grad, axis=0, keepdims=True))
            own_sums[r, :, lanes] = jnp.concatenate(found, 0)

    def backward(lanes):
        for r in range(2):
            ext = jnp.concatenate([grads[r, :, lanes], after[r, :, lanes]], 0)
            total = jnp.zeros((length, CHUNK), F32)
            for k in range(tap_count):
                total = total + param(r, k, lanes) * ext[reach - k : reach - k + length]
            all_g[r, rows(me), lanes] = total.astype(BF16)

    first = pl.ds(0, TAIL)
    left = lax.rem(me + count - 1, count)
    backs, sent_g = [], []
    near.wait_recv()
    for g in range(group_count):
        crossed[g].wait_recv()
        chunks(g, combine)
        back = [
            copy_of(grads.at[r, first, group(g)], after.at[r, :, group(g)], to(left))
            for r in range(2)
        ]
        backs += back

        @pl.when(has_before)
        def _():
            for copy in back:
                copy.start()

        if g == 0:
            for early in range(group_count - 1):
                relay_mixed(early)

        @pl.when(has_after)
        def _():
            for copy in back:
                copy.wait_recv()

        chunks(g, backward)
        beside = []
        for r in range(2):
            here = all_g.at[r, rows(me), group(g)]
            beside.append(launch(here, here, to(sib)))
        for copy in beside:
            copy.wait_recv()
        for j in range(2):
            here = all_g.at[core, rows(chip * 2 + j), group(g)]
            sent_g.append(launch(here, here, to(far)))
    relay_mixed(group_count - 1)
    side_sums = launch(own_sums.at[1 - core], sib_sums, to(sib))

    loads[5].wait()
    loads[6].wait()

    def product(at, lanes, ks):
        total = contract_last(all_g[0, at, ks], weights[0, lanes, ks])
        return total + contract_last(all_g[1, at, ks], weights[1, lanes, ks])

    both = span(chip, 2 * length)
    depth_chunks(lambda lanes: terms.__setitem__(
        (both, lanes), product(both, lanes, pl.ds(0, width))
    ))

    blocks = (me, sib, other * 2, other * 2 + 1)

    def slab(k, index):
        return pl.ds(pl.multiple_of(blocks[k] * length + index * shard, shard), shard)

    pair_copies, line_copies, last_copies = {}, {}, {}

    def send_pair(k):
        for there in range(line):
            to_pair[k, there * shard : (there + 1) * shard, :] = terms[
                slab(k, there * 2 + (1 - y)), :
            ].astype(BF16)
        pair_copies[k] = launch(to_pair.at[k], from_pair.at[k], to_fs(pair))

    def send_line(k):
        pair_copies[k].wait_recv()
        line_copies[k] = []
        for by in sorted(range(1, line), key=lambda by: -min(by, line - by)) + [0]:
            there = lax.rem(z + by, line)
            added = terms[slab(k, there * 2 + y), :] + from_pair[
                k, span(there, shard), :
            ].astype(F32)
            if by == 0:
                kept[k] = added
            else:
                to_line[k, by] = added.astype(BF16)
                line_copies[k].append(
                    (by, launch(to_line.at[k, by], from_line.at[k, by], to_fs(there * 2 + y)))
                )

    a2a = [next(numbers) for _ in range(2)]

    def settle(k):
        total = kept[k]
        for by, copy in line_copies[k]:
            copy.wait_recv()
            total = total + from_line[k, by].astype(F32)
        if k == 0:
            out[:, cols(me)] = total.astype(BF16)
            return
        settled[k] = total.astype(BF16)
        if k == 1:
            last_copies[k] = launch(settled.at[k], out.at[:, cols(me)], to(sib))
        else:
            last_copies[k] = copy_of(
                settled.at[k], out.at[:, cols(me)], to(blocks[k]),
                send_at=a2a[k - 2], receive_at=a2a[0] + core,
            )
            last_copies[k].start()
            pending.append(last_copies[k])

    send_pair(0)
    send_pair(1)

    for copy in mixed_sib:
        copy.wait_recv()
    for copy in mixed_relays:
        copy.wait_recv()
    loads[4].wait()
    own_down[...] = jnp.zeros(own_down.shape, F32)

    def down_step(lanes):
        value = contract_first(columns[:, lanes], all_m[...])
        own_down[...] += jnp.sum(value * value, axis=0, keepdims=True)

    depth_chunks(down_step)
    got_down[me] = own_down[...]
    tp_others = [lax.rem(me + by, count) for by in range(1, count)]
    down_copies = [launch(own_down, got_down.at[me], to(index)) for index in tp_others]

    side_sums.wait_recv()
    chip_sums[...] = own_sums[core] + sib_sums[...]
    cross_sums = launch(chip_sums, far_sums, to(far))
    send_line(0)
    send_line(1)

    own_norms[...] = jnp.zeros(own_norms.shape, F32)

    def norm_group(g):
        def step(lanes):
            for r in range(2):
                value = contract_first(all_g[r, :, lanes], hidden[...])
                own_norms[r : r + 1, :] += jnp.sum(value * value, axis=0, keepdims=True)

        chunks(g, step)

    theirs = span(other, 2 * length)

    def relay_g(g, j):
        sent_g[2 * g + j].wait_recv()
        there = all_g.at[core, rows(other * 2 + j), group(g)]
        return launch(there, there, to(sib))

    for g in range(group_count - 1):
        relays = [relay_g(g, j) for j in range(2)]
        for copy in relays:
            copy.wait_recv()

        def add_group(lanes):
            value = product(theirs, lanes, group(g))
            terms[theirs, lanes] = value if g == 0 else terms[theirs, lanes] + value

        depth_chunks(add_group)
        if g == 0:
            cross_sums.wait_recv()
            sums[core] = chip_sums[...] + far_sums[...]
            side_total = launch(sums.at[core], sums.at[core], to(sib))
            settle(0)
            settle(1)
        norm_group(g)

    side_total.wait_recv()
    total_sums = sums[...]
    own_squares[...] = jnp.broadcast_to(
        jnp.sum(total_sums * total_sums, axis=2, keepdims=True), own_squares.shape
    )
    got_squares[fs] = own_squares[...]
    square_copies = [launch(own_squares, got_squares.at[fs], to_fs(index)) for index in fs_others]

    g = group_count - 1
    for j in range(2):
        relay_g(g, j).wait_recv()
        at = rows(other * 2 + j)

        def add_last(lanes):
            value = product(at, lanes, group(g))
            terms[at, lanes] = value if g == 0 else terms[at, lanes] + value

        depth_chunks(add_last)
        send_pair(2 + j)
    norm_group(g)
    got_norms[fs] = own_norms[...]
    norm_copies = [launch(own_norms, got_norms.at[fs], to_fs(index)) for index in fs_others]
    send_line(2)
    send_line(3)
    settle(2)
    settle(3)
    for copies in (down_copies, square_copies, norm_copies):
        for copy in copies:
            copy.wait_recv()

    def gathered(ref, size):
        total = ref[0]
        for index in range(1, size):
            total = total + ref[index]
        return total

    down_norms[...] = gathered(got_down, count)
    squares[...] = gathered(got_squares, fs_count)
    norms[...] = gathered(got_norms, fs_count)
    last_copies[1].wait_recv()
    for j in range(2):
        copy_of(
            settled.at[0], out.at[:, cols(other * 2 + j)], to(far),
            send_at=a2a[0], receive_at=a2a[j],
        ).wait_recv()
    for copy in pending:
        copy.wait_send()

    @pl.when(has_after)
    def _():
        for copy in halo:
            copy.wait_send()

    @pl.when(has_before)
    def _():
        for copy in backs:
            copy.wait_send()


def gradients(hidden_in, up_act, up_val, cotangent, w_act, w_val, w_down, params):
    length, width = up_act.shape
    depth = w_down.shape[1]
    tp_count, fs_count = lax.axis_size("tp"), lax.axis_size("fs")
    positions = length * tp_count
    shard = length // fs_count
    line = fs_count // 2
    stat_rows = params.shape[0] // 2
    vmem = pl.BlockSpec(memory_space=pltpu.VMEM)
    hbm = pl.BlockSpec(memory_space=pl.ANY)
    block = pltpu.VMEM((length, width), BF16)
    wide = pltpu.VMEM((length, width), F32)
    slots = pltpu.VMEM((4, line * shard, depth), BF16)
    pieces = pltpu.VMEM((4, line, shard, depth), BF16)
    half_sums = pltpu.VMEM((stat_rows, width), F32)
    return pl.pallas_call(
        gradient_kernel,
        out_shape=(
            jax.ShapeDtypeStruct((positions, depth), BF16),
            jax.ShapeDtypeStruct((2, positions, width), BF16),
            jax.ShapeDtypeStruct((positions, width), BF16),
            jax.ShapeDtypeStruct((2, stat_rows, width), F32),
            jax.ShapeDtypeStruct((shard, depth * tp_count), BF16),
            jax.ShapeDtypeStruct((2, depth), F32),
            jax.ShapeDtypeStruct((1, width), F32),
            jax.ShapeDtypeStruct((2, stat_rows, 128), F32),
        ),
        in_specs=[hbm] * 7 + [vmem],
        out_specs=(vmem,) * 8,
        scratch_shapes=[
            pltpu.VMEM(hidden_in.shape, BF16),
            pltpu.VMEM((2, length, width), BF16),
            pltpu.VMEM(cotangent.shape, BF16),
            pltpu.VMEM((2,) + w_act.shape, BF16),
            pltpu.VMEM(w_down.shape, BF16),
            pltpu.VMEM((2, HALO, width), BF16), pltpu.VMEM((2, TAIL, width), F32),
            pltpu.VMEM((2, length, width), F32), wide, wide,
            wide, block, block, block, block, block, block,
            pltpu.VMEM((positions, depth), F32),
            slots, slots, pltpu.VMEM((4, shard, depth), F32), pieces, pieces,
            pltpu.VMEM((4, shard, depth), BF16),
            pltpu.VMEM((2, stat_rows, width), F32), half_sums, half_sums, half_sums,
            pltpu.VMEM((2, depth), F32), pltpu.VMEM((fs_count, 2, depth), F32),
            pltpu.VMEM((1, width), F32), pltpu.VMEM((tp_count, 1, width), F32),
            pltpu.VMEM((2, stat_rows, 128), F32), pltpu.VMEM((fs_count, 2, stat_rows, 128), F32),
            pltpu.SemaphoreType.DMA((COPIES,)), pltpu.SemaphoreType.DMA((COPIES,)),
            pltpu.SemaphoreType.DMA((7,)),
        ],
        compiler_params=pltpu.CompilerParams(
            collective_id=0, has_side_effects=True, vmem_limit_bytes=50 * 1024 * 1024
        ),
    )(hidden_in, up_act, up_val, cotangent, w_act, w_val, w_down, params)


def kernels_fit(up_act, w_down, conv_act):
    length, width = up_act.shape
    fs_count, tp_count = lax.axis_size("fs"), lax.axis_size("tp")
    return (
        tp_count == 4
        and fs_count % 4 == 0
        and width % GROUP == 0
        and width // GROUP > 1
        and w_down.shape[1] % CHUNK == 0
        and length % (16 * fs_count) == 0
        and conv_act.shape[0] - 1 <= TAIL
        and conv_act.shape[0] == 3
        and width * (3 * w_down.shape[1] + 32 * length) * 2 <= 32 * 1024 * 1024
    )


def weight_kernel(
    hidden, all_g, all_m, columns, sums, grad_in, norms, down_norms, squares,
    w_act, w_val, w_down, input_out, conv_a, conv_v, bias_a, bias_v,
    rows_a, rows_v, rows_d, conv_rows,
):
    step = pl.program_id(0)
    per_role = pl.num_programs(0) - all_m.shape[1] // CHUNK
    per_role = per_role // 2
    taps = conv_a.shape[0]

    @pl.when(step < per_role)
    def _():
        w_act[...] = contract_first(hidden[:, span(step, CHUNK)], all_g[0])

    @pl.when(jnp.logical_and(step >= per_role, step < 2 * per_role))
    def _():
        w_val[...] = contract_first(hidden[:, span(step - per_role, CHUNK)], all_g[1])

    @pl.when(step >= 2 * per_role)
    def _():
        w_down[...] = contract_first(all_m[:, span(step - 2 * per_role, CHUNK)], columns[...])

    @pl.when(step == 0)
    def _():
        input_out[...] = grad_in[...]
        conv_a[...] = sums[0, :taps, :]
        conv_v[...] = sums[1, :taps, :]
        bias_a[...] = sums[0, taps : taps + 1, :]
        bias_v[...] = sums[1, taps : taps + 1, :]
        rows_a[...] = norms[0:1, :]
        rows_v[...] = norms[1:2, :]
        rows_d[...] = down_norms[...]
        lane = lax.broadcasted_iota(jnp.int32, (1, 128), 1)
        for r in range(2):
            row = jnp.zeros((1, 128), F32)
            for k in range(taps):
                row = jnp.where(lane == k, squares[r, k : k + 1, :], row)
            conv_rows[r : r + 1, :] = row[:, :taps]


def weight_gradients(hidden_in, all_g, all_m, columns, sums, grad_in, norms, down_norms, squares):
    depth, width = hidden_in.shape[1], all_m.shape[1]
    taps = sums.shape[1] - 1
    per_role, per_down = depth // CHUNK, width // CHUNK
    operands = (hidden_in, all_g, all_m, columns, sums, grad_in, norms, down_norms, squares)

    def whole(shape):
        return pl.BlockSpec(shape, lambda i: (0,) * len(shape))

    small = (
        (grad_in.shape, BF16), ((taps, width), F32), ((taps, width), F32), ((1, width), F32),
        ((1, width), F32), ((1, depth), F32), ((1, depth), F32), ((1, width), F32),
        ((2, taps), F32),
    )
    return pl.pallas_call(
        weight_kernel,
        grid=(2 * per_role + per_down,),
        out_shape=(
            jax.ShapeDtypeStruct((depth, width), F32),
            jax.ShapeDtypeStruct((depth, width), F32),
            jax.ShapeDtypeStruct((width, depth), F32),
            *(jax.ShapeDtypeStruct(shape, dtype) for shape, dtype in small),
        ),
        in_specs=[whole(operand.shape) for operand in operands],
        out_specs=(
            pl.BlockSpec((CHUNK, width), lambda i: (jnp.minimum(i, per_role - 1), 0)),
            pl.BlockSpec(
                (CHUNK, width), lambda i: (jnp.clip(i - per_role, 0, per_role - 1), 0)
            ),
            pl.BlockSpec((CHUNK, depth), lambda i: (jnp.maximum(i - 2 * per_role, 0), 0)),
            *(whole(shape) for shape, _ in small),
        ),
        compiler_params=pltpu.CompilerParams(vmem_limit_bytes=40 * 1024 * 1024),
    )(*operands)


def with_kernels(
    hidden_in, up_act, up_val, cotangent, w_act, w_val, w_down,
    conv_act, conv_val, bias_act, bias_val,
):
    params = jnp.concatenate(
        [conv_act, bias_act[None, :], conv_val, bias_val[None, :]], 0
    ).astype(F32)
    columns, all_g, all_m, sums, grad_in, norms, down_norms, squares = gradients(
        hidden_in, up_act, up_val, cotangent, w_act, w_val, w_down, params
    )
    (
        grad_w_act, grad_w_val, grad_w_down, grad_input, conv_a, conv_v, bias_a, bias_v,
        rows_a, rows_v, rows_d, conv_rows,
    ) = weight_gradients(
        hidden_in, all_g, all_m, columns, sums, grad_in, norms, down_norms, squares
    )
    return (
        grad_input, grad_w_act, grad_w_val, grad_w_down, conv_a, conv_v,
        bias_a.reshape(-1), bias_v.reshape(-1), rows_a.reshape(-1), rows_v.reshape(-1),
        rows_d.reshape(-1), conv_rows,
    )


def passed_along(value, axis, by):
    length = lax.axis_size(axis)
    pairs = [(i, i + by) for i in range(length) if 0 <= i + by < length]
    return lax.ppermute(value, axis, pairs)


def contract_last(left, right):
    return lax.dot_general(
        left, right, (((1,), (1,)), ((), ())), preferred_element_type=jnp.float32
    )


def contract_first(left, right):
    return lax.dot_general(
        left, right, (((0,), (0,)), ((), ())), preferred_element_type=jnp.float32
    )


def conv_ahead(extended, taps, bias, length):
    total = jnp.zeros((length, extended.shape[1]), jnp.float32) + bias.astype(jnp.float32)
    for offset in range(taps.shape[0]):
        total = total + taps[offset].astype(jnp.float32) * extended[offset : offset + length]
    return total


def conv_behind(extended, taps, length):
    reach = taps.shape[0] - 1
    total = jnp.zeros((length, extended.shape[1]), jnp.float32)
    for offset in range(taps.shape[0]):
        total = (
            total
            + taps[offset].astype(jnp.float32) * extended[reach - offset : reach - offset + length]
        )
    return total.astype(jnp.bfloat16)


def tap_grads(grad_pre, extended, tap_count):
    length = grad_pre.shape[0]
    rows = [
        jnp.sum(grad_pre * extended[offset : offset + length], axis=0)
        for offset in range(tap_count)
    ]
    return (jnp.stack(rows, 0), jnp.sum(grad_pre, axis=0))


def per_device(
    hidden_in,
    up_act,
    up_val,
    cotangent,
    w_act,
    w_val,
    w_down,
    conv_act,
    conv_val,
    bias_act,
    bias_val,
):
    if kernels_fit(up_act, w_down, conv_act):
        return with_kernels(
            hidden_in, up_act, up_val, cotangent, w_act, w_val, w_down,
            conv_act, conv_val, bias_act, bias_val,
        )
    local_rows = cotangent.shape[0]
    tap_count = conv_act.shape[0]
    reach = tap_count - 1
    tp_count = lax.axis_size("tp")
    fs_count = lax.axis_size("fs")
    down_whole = lax.all_gather(w_down, "tp", axis=1, tiled=True)
    prev_act, prev_val = passed_along(
        (up_act[local_rows - reach :], up_val[local_rows - reach :]), "tp", 1
    )
    ext_act = jnp.concatenate([prev_act, up_act], 0).astype(jnp.float32)
    ext_val = jnp.concatenate([prev_val, up_val], 0).astype(jnp.float32)
    pre_act = conv_ahead(ext_act, conv_act, bias_act, local_rows)
    pre_val = conv_ahead(ext_val, conv_val, bias_val, local_rows)
    gelu_act, gelu_back = jax.vjp(jax.nn.gelu, pre_act)
    mixed = (gelu_act * pre_val).astype(jnp.bfloat16)
    grad_mixed = contract_last(cotangent, down_whole).astype(jnp.bfloat16)
    grad_mixed = lax.optimization_barrier(grad_mixed).astype(jnp.float32)
    grad_pre_act = gelu_back(grad_mixed * pre_val)[0]
    grad_pre_val = grad_mixed * gelu_act
    next_act, next_val = passed_along((grad_pre_act[:reach], grad_pre_val[:reach]), "tp", -1)
    grad_up_act = conv_behind(jnp.concatenate([grad_pre_act, next_act], 0), conv_act, local_rows)
    grad_up_val = conv_behind(jnp.concatenate([grad_pre_val, next_val], 0), conv_val, local_rows)
    taps_act, sums_act = tap_grads(grad_pre_act, ext_act, tap_count)
    taps_val, sums_val = tap_grads(grad_pre_val, ext_val, tap_count)
    all_up_act, all_up_val, all_mixed = (
        lax.all_gather(grad_up_act, "tp", axis=0, tiled=True),
        lax.all_gather(grad_up_val, "tp", axis=0, tiled=True),
        lax.all_gather(mixed, "tp", axis=0, tiled=True),
    )
    cot_columns = lax.all_to_all(cotangent, "tp", split_axis=1, concat_axis=0, tiled=True)
    grad_w_act = contract_first(hidden_in, all_up_act)
    grad_w_val = contract_first(hidden_in, all_up_val)
    grad_w_down = contract_first(all_mixed, cot_columns)
    shard_rows = local_rows // fs_count
    block_rows = tp_count * shard_rows

    def select_rows(gathered):
        shaped = gathered.reshape(tp_count, fs_count, shard_rows, gathered.shape[1])
        return jnp.transpose(shaped, (1, 0, 2, 3)).reshape(
            lax.axis_size("fs") * block_rows, gathered.shape[1]
        )

    summed = lax.psum_scatter(
        contract_last(select_rows(all_up_act), w_act)
        + contract_last(select_rows(all_up_val), w_val),
        "fs",
        scatter_dimension=0,
        tiled=True,
    ).astype(jnp.bfloat16)
    grad_input = lax.all_to_all(summed, "tp", split_axis=0, concat_axis=1, tiled=True)
    down_squares = jnp.sum(grad_w_down * grad_w_down, axis=1)
    taps_act, taps_val, sums_act, sums_val, rows_down = lax.psum(
        (taps_act, taps_val, sums_act, sums_val, down_squares), "tp"
    )
    tap_squares = jnp.stack(
        [jnp.sum(taps_act * taps_act, axis=1), jnp.sum(taps_val * taps_val, axis=1)], 0
    )
    rows_act, rows_val, conv_rows = lax.psum(
        (
            jnp.sum(grad_w_act * grad_w_act, axis=1),
            jnp.sum(grad_w_val * grad_w_val, axis=1),
            tap_squares,
        ),
        "fs",
    )
    return (
        grad_input,
        grad_w_act,
        grad_w_val,
        grad_w_down,
        taps_act,
        taps_val,
        sums_act,
        sums_val,
        rows_act,
        rows_val,
        rows_down,
        conv_rows,
    )


def solution(mesh):
    return jax.shard_map(
        per_device,
        mesh=mesh,
        in_specs=(
            P(None, "tp"),
            P("tp", "fs"),
            P("tp", "fs"),
            P("tp", None),
            P("tp", "fs"),
            P("tp", "fs"),
            P("fs", "tp"),
            P(None, "fs"),
            P(None, "fs"),
            P("fs"),
            P("fs"),
        ),
        out_specs=(
            P(("tp", "fs"), None),
            P("tp", "fs"),
            P("tp", "fs"),
            P("fs", "tp"),
            P(None, "fs"),
            P(None, "fs"),
            P("fs"),
            P("fs"),
            P("tp"),
            P("tp"),
            P("fs"),
            P(),
        ),
        check_vma=False,
    )
```

```python
import itertools

import jax
import jax.numpy as jnp
from jax import lax
from jax.experimental import pallas as pl
from jax.experimental.pallas import tpu as pltpu
from jax.sharding import PartitionSpec as P

MESH = pl.DeviceIdType.MESH
F32 = jnp.float32
BF16 = jnp.bfloat16
CHUNK = 256
GROUP = 512
HALO = 16
TAIL = 8
COPIES = 112
ROWS = 512
SLOTS = 3
ROOT_TWO_OVER_PI = 0.7978845608028654
CUBIC = 0.044715


def span(index, size):
    return pl.ds(pl.multiple_of(index * size, size), size)


def gradient_kernel(
    hidden_hbm, up_a_hbm, up_v_hbm, cot_hbm, w_a_hbm, w_v_hbm, down_hbm,
    taps_a_hbm, taps_v_hbm, bias_a_hbm, bias_v_hbm,
    columns, all_g, all_m, sums, out, norms, down_norms, squares,
    hidden, up, cot, weights, down, taps_a, taps_v, bias_a, bias_v, params,
    before, after, grads, gated, factor,
    own, to_sib, from_sib, to_sib_far, from_sib_far, to_far, from_far,
    terms, to_pair, from_pair, kept, to_line, from_line, settled,
    own_sums, sib_sums, chip_sums, far_sums, own_norms, got_norms, own_down, got_down,
    own_squares, got_squares,
    send, receive, loaded,
):
    me, fs = lax.axis_index("tp"), lax.axis_index("fs")
    count, fs_count = lax.axis_size("tp"), lax.axis_size("fs")
    chip, core = me // 2, me % 2
    other = 1 - chip
    sib, far, diag = chip * 2 + (1 - core), other * 2 + core, other * 2 + (1 - core)
    line = fs_count // 2
    z, y = fs // 2, fs % 2
    pair = z * 2 + (1 - y)
    z_mate = z + 1 - 2 * (z % 2)
    length, width = up.shape[1:]
    depth = down.shape[1]
    tap_count = taps_a.shape[0]
    reach = tap_count - 1
    group_count = width // GROUP
    shard = out.shape[0]
    quarter = length // 4

    def to(index):
        return {"tp": index}

    def to_fs(index):
        return {"fs": index}

    fs_others = [lax.rem(fs + by, fs_count) for by in range(1, fs_count)]
    numbers = itertools.count()
    pending = []

    def copy_of(source, target, where, send_at=None, receive_at=None):
        number = next(numbers) if send_at is None else send_at
        assert number < COPIES
        return pltpu.make_async_remote_copy(
            src_ref=source,
            dst_ref=target,
            send_sem=send.at[number],
            recv_sem=receive.at[number if receive_at is None else receive_at],
            device_id=where,
            device_id_type=MESH,
        )

    def launch(source, target, where):
        copy = copy_of(source, target, where)
        copy.start()
        pending.append(copy)
        return copy

    def rows(index):
        return span(index, length)

    def cols(index):
        return span(index, depth)

    def group(g):
        return pl.ds(g * GROUP, GROUP)

    def chunks(g, step):
        def at(i, carry):
            step(pl.ds(pl.multiple_of(g * GROUP + i * CHUNK, CHUNK), CHUNK))
            return carry

        lax.fori_loop(0, GROUP // CHUNK, at, 0)

    def depth_chunks(step, part=0, parts=1):
        per_part = depth // (CHUNK * parts)

        def at(i, carry):
            step(span(part * per_part + i, CHUNK))
            return carry

        lax.fori_loop(0, per_part, at, 0)

    sources = (
        (up_a_hbm, up.at[0]), (up_v_hbm, up.at[1]), (cot_hbm, cot), (taps_a_hbm, taps_a),
        (taps_v_hbm, taps_v), (bias_a_hbm, bias_a), (bias_v_hbm, bias_v), (down_hbm, down),
        (hidden_hbm, hidden), (w_a_hbm, weights.at[0]), (w_v_hbm, weights.at[1]),
    )
    loads = [
        pltpu.make_async_copy(source, target, loaded.at[i])
        for i, (source, target) in enumerate(sources)
    ]
    for load in loads:
        load.start()

    barrier = pltpu.get_barrier_semaphore()
    everyone = [to(sib), to(far), to(diag)] + [to_fs(index) for index in fs_others]
    for where in everyone:
        pl.semaphore_signal(barrier, inc=1, device_id=where, device_id_type=MESH)
    pl.semaphore_wait(barrier, len(everyone))

    loads[0].wait()
    loads[1].wait()
    has_before, has_after = me > 0, me < count - 1
    last = pl.ds(length - HALO, HALO)
    halo = [copy_of(up.at[r, last, :], before.at[r], to(lax.rem(me + 1, count))) for r in range(2)]

    @pl.when(has_after)
    def _():
        for copy in halo:
            copy.start()

    @pl.when(jnp.logical_not(has_before))
    def _():
        before[...] = jnp.zeros(before.shape, before.dtype)

    @pl.when(jnp.logical_not(has_after))
    def _():
        after[...] = jnp.zeros(after.shape, after.dtype)

    loads[2].wait()
    for load in loads[3:7]:
        load.wait()
    for r, (taps, bias) in enumerate(((taps_a, bias_a), (taps_v, bias_v))):
        at = r * (tap_count + 1)
        params[at : at + tap_count, :] = taps[...].astype(F32)
        params[at + tap_count : at + tap_count + 1, :] = bias[...].astype(F32)[None, :]
    mine = span((z % 2) * 2 + y, quarter)

    def quarter_of(index):
        at = index * length + ((z % 2) * 2 + y) * quarter
        return columns.at[pl.ds(pl.multiple_of(at, quarter), quarter), :]

    cot_diag = launch(cot.at[mine, cols(diag)], quarter_of(me), to(diag))
    cot_far = launch(cot.at[mine, cols(far)], quarter_of(me), to(far))
    cot_sib = launch(cot.at[:, cols(sib)], columns.at[rows(me), :], to(sib))
    columns[rows(me), :] = cot[:, cols(me)]

    def share(index):
        mates = (pair, z_mate * 2 + y, z_mate * 2 + (1 - y))
        return [launch(quarter_of(index), quarter_of(index), to_fs(mate)) for mate in mates]

    def shifted(r, lanes):
        ext = jnp.concatenate([before[r, :, lanes].astype(F32), up[r, :, lanes].astype(F32)], 0)
        return [ext[HALO - reach + k : HALO - reach + k + length] for k in range(tap_count)]

    def param(r, k, lanes):
        at = r * (tap_count + 1) + k
        return params[at : at + 1, lanes]

    def forward(lanes):
        pre = []
        for r in range(2):
            taken = shifted(r, lanes)
            total = jnp.broadcast_to(param(r, tap_count, lanes), (length, CHUNK))
            for k in range(tap_count):
                total = total + param(r, k, lanes) * taken[k]
            pre.append(total)
        pre_a, pre_v = pre
        square = pre_a * pre_a
        bent = jnp.tanh(ROOT_TWO_OVER_PI * pre_a * (1.0 + CUBIC * square))
        half = 0.5 * (1.0 + bent)
        gelu = pre_a * half
        slope = half + 0.5 * pre_a * (1.0 - bent * bent) * (
            ROOT_TWO_OVER_PI * (1.0 + 3.0 * CUBIC * square)
        )
        all_m[rows(me), lanes] = (gelu * pre_v).astype(BF16)
        gated[:, lanes] = gelu
        factor[:, lanes] = pre_v * slope

    mixed_far, mixed_sib = [], []

    def spread_mixed(g):
        here = all_m.at[rows(me), group(g)]
        mixed_far.append(launch(here, here, to(far)))
        mixed_sib.append(launch(here, here, to(sib)))

    @pl.when(has_before)
    def _():
        for copy in halo:
            copy.wait_recv()

    for g in range(group_count):
        chunks(g, forward)
        spread_mixed(g)
        if g == 0:
            cot_diag.wait_recv()
            shared_diag = share(diag)
        if g == 1:
            cot_far.wait_recv()
            shared_far = share(far)

    loads[7].wait()

    def partial(index, g, finish):
        def step(lanes):
            finish(lanes, contract_last(columns[rows(index), :], down[lanes, :]))

        chunks(g, step)

    def keep(target):
        def finish(lanes, value):
            target[:, lanes] = value.astype(target.dtype)

        return finish

    def add_far(lanes, value):
        to_far[:, lanes] = (value + from_sib_far[:, lanes].astype(F32)).astype(BF16)

    for g in range(group_count):
        partial(me, g, keep(own))
    cot_sib.wait_recv()
    for g in range(group_count):
        partial(sib, g, keep(to_sib))
    near = launch(to_sib, from_sib, to(sib))
    relayed, crossed = [], []

    def diag_part(g):
        partial(diag, g, keep(to_sib_far))
        relayed.append(launch(to_sib_far.at[:, group(g)], from_sib_far.at[:, group(g)], to(sib)))

    def far_part(g):
        relayed[g].wait_recv()
        partial(far, g, add_far)
        crossed.append(launch(to_far.at[:, group(g)], from_far.at[:, group(g)], to(far)))

    for copy in shared_diag:
        copy.wait_recv()
    diag_part(0)
    for g in range(1, group_count):
        diag_part(g)
        if g == 1:
            for copy in shared_far:
                copy.wait_recv()
        far_part(g - 1)
    far_part(group_count - 1)

    mixed_relays = []

    def relay_mixed(g):
        mixed_far[g].wait_recv()
        there = all_m.at[rows(far), group(g)]
        mixed_relays.append(launch(there, there, to(sib)))

    def combine(lanes):
        total = own[:, lanes] + from_sib[:, lanes].astype(F32) + from_far[:, lanes].astype(F32)
        grad_mixed = total.astype(BF16).astype(F32)
        for r, scale in ((0, factor), (1, gated)):
            pre_grad = grad_mixed * scale[:, lanes]
            grads[r, :, lanes] = pre_grad
            found = [
                jnp.sum(pre_grad * taken, axis=0, keepdims=True) for taken in shifted(r, lanes)
            ]
            found.append(jnp.sum(pre_grad, axis=0, keepdims=True))
            own_sums[r, :, lanes] = jnp.concatenate(found, 0)

    def backward(lanes):
        for r in range(2):
            ext = jnp.concatenate([grads[r, :, lanes], after[r, :, lanes]], 0)
            total = jnp.zeros((length, CHUNK), F32)
            for k in range(tap_count):
                total = total + param(r, k, lanes) * ext[reach - k : reach - k + length]
            all_g[r, rows(me), lanes] = total.astype(BF16)

    first = pl.ds(0, TAIL)
    left = lax.rem(me + count - 1, count)
    final = group_count - 1
    backs, sent_g = [], {}

    def cross(g, j):
        here = all_g.at[core, rows(chip * 2 + j), group(g)]
        sent_g[g, j] = launch(here, here, to(far))

    near.wait_recv()
    for g in range(group_count):
        crossed[g].wait_recv()
        chunks(g, combine)
        back = [
            copy_of(grads.at[r, first, group(g)], after.at[r, :, group(g)], to(left))
            for r in range(2)
        ]
        backs += back

        @pl.when(has_before)
        def _():
            for copy in back:
                copy.start()

        if g == 0:
            for early in range(group_count - 1):
                relay_mixed(early)

        @pl.when(has_after)
        def _():
            for copy in back:
                copy.wait_recv()

        chunks(g, backward)
        beside = []
        for r in range(2):
            here = all_g.at[r, rows(me), group(g)]
            beside.append(launch(here, here, to(sib)))
        for copy in beside:
            copy.wait_recv()
        cross(g, 0)
        if g < final - 1:
            cross(g, 1)
    cross(final - 1, 1)
    cross(final, 1)
    relay_mixed(group_count - 1)
    side_sums = launch(own_sums.at[1 - core], sib_sums, to(sib))

    loads[9].wait()
    loads[10].wait()

    def product(at, lanes, ks):
        total = contract_last(all_g[0, at, ks], weights[0, lanes, ks])
        return total + contract_last(all_g[1, at, ks], weights[1, lanes, ks])

    both = span(chip, 2 * length)
    depth_chunks(lambda lanes: terms.__setitem__(
        (both, lanes), product(both, lanes, pl.ds(0, width))
    ))

    blocks = (me, sib, other * 2, other * 2 + 1)

    def slab(k, index):
        return pl.ds(pl.multiple_of(blocks[k] * length + index * shard, shard), shard)

    pair_copies, line_copies, last_copies = {}, {}, {}
    parts = 2 if depth % (2 * CHUNK) == 0 else 1
    whole = pl.ds(0, depth)

    def part_of(part):
        return pl.ds(part * (depth // parts), depth // parts)

    def send_pair(k, part=None):
        at = whole if part is None else part_of(part)
        for there in range(line):
            to_pair[k, there * shard : (there + 1) * shard, at] = terms[
                slab(k, there * 2 + (1 - y)), at
            ].astype(BF16)
        pair_copies[k, part] = launch(to_pair.at[k, :, at], from_pair.at[k, :, at], to_fs(pair))

    def send_line(k, part=None):
        at = whole if part is None else part_of(part)
        pair_copies[k, part].wait_recv()
        line_copies[k, part] = []
        for by in sorted(range(1, line), key=lambda by: -min(by, line - by)) + [0]:
            there = lax.rem(z + by, line)
            added = terms[slab(k, there * 2 + y), at] + from_pair[
                k, span(there, shard), at
            ].astype(F32)
            if by == 0:
                kept[k, :, at] = added
            else:
                to_line[k, by, :, at] = added.astype(BF16)
                line_copies[k, part].append((by, launch(
                    to_line.at[k, by, :, at], from_line.at[k, by, :, at], to_fs(there * 2 + y)
                )))

    a2a = [next(numbers) for _ in range(2)]

    def settle(k, split=(None,)):
        for part in split:
            at = whole if part is None else part_of(part)
            total = kept[k, :, at]
            for by, copy in line_copies[k, part]:
                copy.wait_recv()
                total = total + from_line[k, by, :, at].astype(F32)
            settled[k, :, at] = total.astype(BF16)
        if k == 0:
            out[:, cols(me)] = settled[k]
        elif k == 1:
            last_copies[k] = launch(settled.at[k], out.at[:, cols(me)], to(sib))
        else:
            last_copies[k] = copy_of(
                settled.at[k], out.at[:, cols(me)], to(blocks[k]),
                send_at=a2a[k - 2], receive_at=a2a[0] + core,
            )
            last_copies[k].start()
            pending.append(last_copies[k])

    send_pair(0)
    send_pair(1)

    for copy in mixed_sib:
        copy.wait_recv()
    for copy in mixed_relays:
        copy.wait_recv()
    loads[8].wait()
    own_down[...] = jnp.zeros(own_down.shape, F32)

    def down_step(lanes):
        value = contract_first(columns[:, lanes], all_m[...])
        own_down[...] += jnp.sum(value * value, axis=0, keepdims=True)

    depth_chunks(down_step)
    got_down[me] = own_down[...]
    tp_others = [lax.rem(me + by, count) for by in range(1, count)]
    down_copies = [launch(own_down, got_down.at[me], to(index)) for index in tp_others]

    side_sums.wait_recv()
    chip_sums[...] = own_sums[core] + sib_sums[...]
    cross_sums = launch(chip_sums, far_sums, to(far))
    send_line(0)
    send_line(1)

    own_norms[...] = jnp.zeros(own_norms.shape, F32)

    def norm_group(g):
        def step(lanes):
            for r in range(2):
                value = contract_first(all_g[r, :, lanes], hidden[...])
                own_norms[r : r + 1, :] += jnp.sum(value * value, axis=0, keepdims=True)

        chunks(g, step)

    theirs = span(other, 2 * length)

    def relay_g(g, j):
        sent_g[g, j].wait_recv()
        there = all_g.at[core, rows(other * 2 + j), group(g)]
        return launch(there, there, to(sib))

    def take(*which):
        for copy in [relay_g(g, j) for g, j in which]:
            copy.wait_recv()

    def add(at, ks, fresh, part=0, split=1):
        def step(lanes):
            value = product(at, lanes, ks)
            terms[at, lanes] = value if fresh else terms[at, lanes] + value

        depth_chunks(step, part, split)

    for g in range(final - 1):
        take((g, 0), (g, 1))
        add(theirs, group(g), g == 0)
        if g == 0:
            cross_sums.wait_recv()
            sums[core] = chip_sums[...] + far_sums[...]
            side_total = launch(sums.at[core], sums.at[core], to(sib))
            settle(0)
            settle(1)
    for g in range(final - 1):
        norm_group(g)
    take((final - 1, 0), (final, 0))
    add(rows(other * 2), pl.ds((final - 1) * GROUP, 2 * GROUP), final == 1)
    send_pair(2)
    side_total.wait_recv()
    total_sums = sums[...]
    own_squares[...] = jnp.broadcast_to(
        jnp.sum(total_sums * total_sums, axis=2, keepdims=True), own_squares.shape
    )
    got_squares[fs] = own_squares[...]
    square_copies = [launch(own_squares, got_squares.at[fs], to_fs(index)) for index in fs_others]
    take((final - 1, 1))
    add(rows(other * 2 + 1), group(final - 1), final == 1)
    send_line(2)
    norm_group(final - 1)
    take((final, 1))
    for part in range(parts):
        add(rows(other * 2 + 1), group(final), False, part, parts)
        send_pair(3, part)
    norm_group(final)
    got_norms[fs] = own_norms[...]
    norm_copies = [launch(own_norms, got_norms.at[fs], to_fs(index)) for index in fs_others]
    for part in range(parts):
        send_line(3, part)
    settle(2)
    settle(3, range(parts))
    for copies in (down_copies, square_copies, norm_copies):
        for copy in copies:
            copy.wait_recv()

    def gathered(ref, size):
        total = ref[0]
        for index in range(1, size):
            total = total + ref[index]
        return total

    down_norms[...] = gathered(got_down, count)
    squares[...] = gathered(got_squares, fs_count)
    norms[...] = gathered(got_norms, fs_count)
    last_copies[1].wait_recv()
    for j in range(2):
        copy_of(
            settled.at[0], out.at[:, cols(other * 2 + j)], to(far),
            send_at=a2a[0], receive_at=a2a[j],
        ).wait_recv()
    for copy in pending:
        copy.wait_send()

    @pl.when(has_after)
    def _():
        for copy in halo:
            copy.wait_send()

    @pl.when(has_before)
    def _():
        for copy in backs:
            copy.wait_send()


def gradients(
    hidden_in, up_act, up_val, cotangent, w_act, w_val, w_down,
    conv_act, conv_val, bias_act, bias_val,
):
    length, width = up_act.shape
    depth = w_down.shape[1]
    tp_count, fs_count = lax.axis_size("tp"), lax.axis_size("fs")
    positions = length * tp_count
    shard = length // fs_count
    line = fs_count // 2
    stat_rows = conv_act.shape[0] + 1
    vmem = pl.BlockSpec(memory_space=pltpu.VMEM)
    hbm = pl.BlockSpec(memory_space=pltpu.HBM)
    block = pltpu.VMEM((length, width), BF16)
    wide = pltpu.VMEM((length, width), F32)
    slots = pltpu.VMEM((4, line * shard, depth), BF16)
    pieces = pltpu.VMEM((4, line, shard, depth), BF16)
    half_sums = pltpu.VMEM((stat_rows, width), F32)
    return pl.pallas_call(
        gradient_kernel,
        out_shape=(
            jax.ShapeDtypeStruct((positions, depth), BF16),
            jax.ShapeDtypeStruct((2, positions, width), BF16),
            jax.ShapeDtypeStruct((positions, width), BF16),
            jax.ShapeDtypeStruct((2, stat_rows, width), F32),
            jax.ShapeDtypeStruct((shard, depth * tp_count), BF16),
            jax.ShapeDtypeStruct((2, depth), F32),
            jax.ShapeDtypeStruct((1, width), F32),
            jax.ShapeDtypeStruct((2, stat_rows, 128), F32),
        ),
        in_specs=[hbm] * 11,
        out_specs=(vmem,) * 8,
        scratch_shapes=[
            pltpu.VMEM(hidden_in.shape, BF16),
            pltpu.VMEM((2, length, width), BF16),
            pltpu.VMEM(cotangent.shape, BF16),
            pltpu.VMEM((2,) + w_act.shape, BF16),
            pltpu.VMEM(w_down.shape, BF16),
            pltpu.VMEM(conv_act.shape, BF16), pltpu.VMEM(conv_val.shape, BF16),
            pltpu.VMEM((width,), BF16), pltpu.VMEM((width,), BF16),
            pltpu.VMEM((2 * stat_rows, width), F32),
            pltpu.VMEM((2, HALO, width), BF16), pltpu.VMEM((2, TAIL, width), F32),
            pltpu.VMEM((2, length, width), F32), wide, wide,
            wide, block, block, block, block, block, block,
            pltpu.VMEM((positions, depth), F32),
            slots, slots, pltpu.VMEM((4, shard, depth), F32), pieces, pieces,
            pltpu.VMEM((4, shard, depth), BF16),
            pltpu.VMEM((2, stat_rows, width), F32), half_sums, half_sums, half_sums,
            pltpu.VMEM((2, depth), F32), pltpu.VMEM((fs_count, 2, depth), F32),
            pltpu.VMEM((1, width), F32), pltpu.VMEM((tp_count, 1, width), F32),
            pltpu.VMEM((2, stat_rows, 128), F32), pltpu.VMEM((fs_count, 2, stat_rows, 128), F32),
            pltpu.SemaphoreType.DMA((COPIES,)), pltpu.SemaphoreType.DMA((COPIES,)),
            pltpu.SemaphoreType.DMA((11,)),
        ],
        compiler_params=pltpu.CompilerParams(
            collective_id=0, has_side_effects=True, vmem_limit_bytes=34 * 1024 * 1024
        ),
    )(*(
        pltpu.with_memory_space_constraint(operand, pltpu.HBM)
        for operand in (
            hidden_in, up_act, up_val, cotangent, w_act, w_val, w_down,
            conv_act, conv_val, bias_act, bias_val,
        )
    ))


def kernels_fit(up_act, w_down, conv_act):
    length, width = up_act.shape
    fs_count, tp_count = lax.axis_size("fs"), lax.axis_size("tp")
    return (
        tp_count == 4
        and fs_count % 4 == 0
        and width % GROUP == 0
        and width // GROUP > 2
        and w_down.shape[1] % ROWS == 0
        and width % ROWS == 0
        and length % (16 * fs_count) == 0
        and conv_act.shape[0] - 1 <= TAIL
        and conv_act.shape[0] == 3
        and width * (3 * w_down.shape[1] + 32 * length) * 2 <= 32 * 1024 * 1024
    )


def weight_kernel(
    hidden, all_g, all_m, columns, sums, grad_in, norms, down_norms, squares,
    w_act, w_val, w_down, input_out, conv_a, conv_v, bias_a, bias_v,
    rows_a, rows_v, rows_d, conv_rows,
    blocks, held_conv, held_rows, held_a, held_v, held_d, held_rows_a, held_rows_v,
    done, small_done,
):
    taps = conv_a.shape[0]
    depth, width = hidden.shape[1], all_m.shape[1]
    for r in range(2):
        held_conv[r] = sums[r, :taps, :]
    held_a[...] = sums[0, taps, :]
    held_v[...] = sums[1, taps, :]
    held_d[...] = down_norms[0, :]
    held_rows_a[...] = norms[0, :]
    held_rows_v[...] = norms[1, :]
    lane = lax.broadcasted_iota(jnp.int32, (1, 128), 1)
    for r in range(2):
        row = jnp.zeros((1, 128), F32)
        for k in range(taps):
            row = jnp.where(lane == k, squares[r, k : k + 1, :], row)
        held_rows[r : r + 1, :] = row[:, :taps]
    pairs = (
        (grad_in, input_out), (held_conv.at[0], conv_a), (held_conv.at[1], conv_v),
        (held_a, bias_a), (held_v, bias_v), (held_rows_a, rows_a),
        (held_rows_v, rows_v), (held_d, rows_d), (held_rows, conv_rows),
    )
    flying = [
        pltpu.make_async_copy(source, target, small_done.at[i])
        for i, (source, target) in enumerate(pairs)
    ]
    for copy in flying:
        copy.start()
    jobs = [(hidden, all_g.at[0], w_act, at) for at in range(0, depth, ROWS)]
    jobs += [(hidden, all_g.at[1], w_val, at) for at in range(0, depth, ROWS)]
    jobs += [(all_m, columns, w_down, at) for at in range(0, width, ROWS)]
    stored = []
    for number, (left, right, target, at) in enumerate(jobs):
        slot = number % SLOTS
        if number >= SLOTS:
            stored[number - SLOTS].wait()
        size = right.shape[1]
        blocks[slot, :, :size] = contract_first(left[:, at : at + ROWS], right[...])
        stored.append(pltpu.make_async_copy(
            blocks.at[slot, :, pl.ds(0, size)], target.at[pl.ds(at, ROWS), :], done.at[slot]
        ))
        stored[number].start()
    for copy in stored[-SLOTS:] + flying:
        copy.wait()


def weight_gradients(hidden_in, all_g, all_m, columns, sums, grad_in, norms, down_norms, squares):
    depth, width = hidden_in.shape[1], all_m.shape[1]
    taps = sums.shape[1] - 1
    operands = (hidden_in, all_g, all_m, columns, sums, grad_in, norms, down_norms, squares)
    shapes = (
        (depth, width), (depth, width), (width, depth), None, (taps, width), (taps, width),
        (width,), (width,), (depth,), (depth,), (width,), (2, taps),
    )
    return pl.pallas_call(
        weight_kernel,
        out_shape=tuple(
            jax.ShapeDtypeStruct(grad_in.shape, BF16) if shape is None
            else jax.ShapeDtypeStruct(shape, F32)
            for shape in shapes
        ),
        in_specs=[pl.BlockSpec(memory_space=pltpu.VMEM)] * len(operands),
        out_specs=(pl.BlockSpec(memory_space=pltpu.HBM),) * len(shapes),
        scratch_shapes=[
            pltpu.VMEM((SLOTS, ROWS, max(depth, width)), F32),
            pltpu.VMEM((2, taps, width), F32), pltpu.VMEM((2, taps), F32),
            pltpu.VMEM((width,), F32), pltpu.VMEM((width,), F32), pltpu.VMEM((width,), F32),
            pltpu.VMEM((depth,), F32), pltpu.VMEM((depth,), F32),
            pltpu.SemaphoreType.DMA((SLOTS,)), pltpu.SemaphoreType.DMA((9,)),
        ],
        compiler_params=pltpu.CompilerParams(vmem_limit_bytes=24 * 1024 * 1024),
    )(*operands)


def with_kernels(
    hidden_in, up_act, up_val, cotangent, w_act, w_val, w_down,
    conv_act, conv_val, bias_act, bias_val,
):
    columns, all_g, all_m, sums, grad_in, norms, down_norms, squares = gradients(
        hidden_in, up_act, up_val, cotangent, w_act, w_val, w_down,
        conv_act, conv_val, bias_act, bias_val,
    )
    (
        grad_w_act, grad_w_val, grad_w_down, grad_input, conv_a, conv_v, bias_a, bias_v,
        rows_a, rows_v, rows_d, conv_rows,
    ) = weight_gradients(
        hidden_in, all_g, all_m, columns, sums, grad_in, norms, down_norms, squares
    )
    return (
        grad_input, grad_w_act, grad_w_val, grad_w_down, conv_a, conv_v,
        bias_a, bias_v, rows_a, rows_v, rows_d, conv_rows,
    )


def passed_along(value, axis, by):
    length = lax.axis_size(axis)
    pairs = [(i, i + by) for i in range(length) if 0 <= i + by < length]
    return lax.ppermute(value, axis, pairs)


def contract_last(left, right):
    return lax.dot_general(
        left, right, (((1,), (1,)), ((), ())), preferred_element_type=jnp.float32
    )


def contract_first(left, right):
    return lax.dot_general(
        left, right, (((0,), (0,)), ((), ())), preferred_element_type=jnp.float32
    )


def conv_ahead(extended, taps, bias, length):
    total = jnp.zeros((length, extended.shape[1]), jnp.float32) + bias.astype(jnp.float32)
    for offset in range(taps.shape[0]):
        total = total + taps[offset].astype(jnp.float32) * extended[offset : offset + length]
    return total


def conv_behind(extended, taps, length):
    reach = taps.shape[0] - 1
    total = jnp.zeros((length, extended.shape[1]), jnp.float32)
    for offset in range(taps.shape[0]):
        total = (
            total
            + taps[offset].astype(jnp.float32) * extended[reach - offset : reach - offset + length]
        )
    return total.astype(jnp.bfloat16)


def tap_grads(grad_pre, extended, tap_count):
    length = grad_pre.shape[0]
    rows = [
        jnp.sum(grad_pre * extended[offset : offset + length], axis=0)
        for offset in range(tap_count)
    ]
    return (jnp.stack(rows, 0), jnp.sum(grad_pre, axis=0))


def per_device(
    hidden_in,
    up_act,
    up_val,
    cotangent,
    w_act,
    w_val,
    w_down,
    conv_act,
    conv_val,
    bias_act,
    bias_val,
):
    if kernels_fit(up_act, w_down, conv_act):
        return with_kernels(
            hidden_in, up_act, up_val, cotangent, w_act, w_val, w_down,
            conv_act, conv_val, bias_act, bias_val,
        )
    local_rows = cotangent.shape[0]
    tap_count = conv_act.shape[0]
    reach = tap_count - 1
    tp_count = lax.axis_size("tp")
    fs_count = lax.axis_size("fs")
    down_whole = lax.all_gather(w_down, "tp", axis=1, tiled=True)
    prev_act, prev_val = passed_along(
        (up_act[local_rows - reach :], up_val[local_rows - reach :]), "tp", 1
    )
    ext_act = jnp.concatenate([prev_act, up_act], 0).astype(jnp.float32)
    ext_val = jnp.concatenate([prev_val, up_val], 0).astype(jnp.float32)
    pre_act = conv_ahead(ext_act, conv_act, bias_act, local_rows)
    pre_val = conv_ahead(ext_val, conv_val, bias_val, local_rows)
    gelu_act, gelu_back = jax.vjp(jax.nn.gelu, pre_act)
    mixed = (gelu_act * pre_val).astype(jnp.bfloat16)
    grad_mixed = contract_last(cotangent, down_whole).astype(jnp.bfloat16)
    grad_mixed = lax.optimization_barrier(grad_mixed).astype(jnp.float32)
    grad_pre_act = gelu_back(grad_mixed * pre_val)[0]
    grad_pre_val = grad_mixed * gelu_act
    next_act, next_val = passed_along((grad_pre_act[:reach], grad_pre_val[:reach]), "tp", -1)
    grad_up_act = conv_behind(jnp.concatenate([grad_pre_act, next_act], 0), conv_act, local_rows)
    grad_up_val = conv_behind(jnp.concatenate([grad_pre_val, next_val], 0), conv_val, local_rows)
    taps_act, sums_act = tap_grads(grad_pre_act, ext_act, tap_count)
    taps_val, sums_val = tap_grads(grad_pre_val, ext_val, tap_count)
    all_up_act, all_up_val, all_mixed = (
        lax.all_gather(grad_up_act, "tp", axis=0, tiled=True),
        lax.all_gather(grad_up_val, "tp", axis=0, tiled=True),
        lax.all_gather(mixed, "tp", axis=0, tiled=True),
    )
    cot_columns = lax.all_to_all(cotangent, "tp", split_axis=1, concat_axis=0, tiled=True)
    grad_w_act = contract_first(hidden_in, all_up_act)
    grad_w_val = contract_first(hidden_in, all_up_val)
    grad_w_down = contract_first(all_mixed, cot_columns)
    shard_rows = local_rows // fs_count
    block_rows = tp_count * shard_rows

    def select_rows(gathered):
        shaped = gathered.reshape(tp_count, fs_count, shard_rows, gathered.shape[1])
        return jnp.transpose(shaped, (1, 0, 2, 3)).reshape(
            lax.axis_size("fs") * block_rows, gathered.shape[1]
        )

    summed = lax.psum_scatter(
        contract_last(select_rows(all_up_act), w_act)
        + contract_last(select_rows(all_up_val), w_val),
        "fs",
        scatter_dimension=0,
        tiled=True,
    ).astype(jnp.bfloat16)
    grad_input = lax.all_to_all(summed, "tp", split_axis=0, concat_axis=1, tiled=True)
    down_squares = jnp.sum(grad_w_down * grad_w_down, axis=1)
    taps_act, taps_val, sums_act, sums_val, rows_down = lax.psum(
        (taps_act, taps_val, sums_act, sums_val, down_squares), "tp"
    )
    tap_squares = jnp.stack(
        [jnp.sum(taps_act * taps_act, axis=1), jnp.sum(taps_val * taps_val, axis=1)], 0
    )
    rows_act, rows_val, conv_rows = lax.psum(
        (
            jnp.sum(grad_w_act * grad_w_act, axis=1),
            jnp.sum(grad_w_val * grad_w_val, axis=1),
            tap_squares,
        ),
        "fs",
    )
    return (
        grad_input,
        grad_w_act,
        grad_w_val,
        grad_w_down,
        taps_act,
        taps_val,
        sums_act,
        sums_val,
        rows_act,
        rows_val,
        rows_down,
        conv_rows,
    )


def solution(mesh):
    return jax.shard_map(
        per_device,
        mesh=mesh,
        in_specs=(
            P(None, "tp"),
            P("tp", "fs"),
            P("tp", "fs"),
            P("tp", None),
            P("tp", "fs"),
            P("tp", "fs"),
            P("fs", "tp"),
            P(None, "fs"),
            P(None, "fs"),
            P("fs"),
            P("fs"),
        ),
        out_specs=(
            P(("tp", "fs"), None),
            P("tp", "fs"),
            P("tp", "fs"),
            P("fs", "tp"),
            P(None, "fs"),
            P(None, "fs"),
            P("fs"),
            P("fs"),
            P("tp"),
            P("tp"),
            P("fs"),
            P(),
        ),
        check_vma=False,
    )
```

```python
import itertools

import jax
import jax.numpy as jnp
from jax import lax
from jax.experimental import pallas as pl
from jax.experimental.pallas import tpu as pltpu
from jax.sharding import PartitionSpec as P

MESH = pl.DeviceIdType.MESH
F32 = jnp.float32
BF16 = jnp.bfloat16
CHUNK = 256
GROUP = 512
HALO = 8
TAIL = 8
COPIES = 144
ROWS = 512
SLOTS = 3
ROOT_TWO_OVER_PI = 0.7978845608028654
CUBIC = 0.044715


def span(index, size):
    return pl.ds(pl.multiple_of(index * size, size), size)


def gradient_kernel(
    hidden_hbm, up_a_hbm, up_v_hbm, cot_hbm, w_a_hbm, w_v_hbm, down_hbm,
    taps_a_hbm, taps_v_hbm, bias_a_hbm, bias_v_hbm,
    columns, all_g, all_m, sums, out, norms, down_norms, squares,
    hidden, up, cot, weights, down, taps_a, taps_v, bias_a, bias_v, params,
    before, after, grads, gated, factor,
    own, to_sib, from_sib, to_sib_far, from_sib_far, to_far, from_far,
    terms, to_pair, from_pair, kept, to_line, from_line, settled, arrived,
    own_sums, sib_sums, chip_sums, far_sums, own_norms, got_norms, own_down, got_down,
    own_squares, got_squares,
    send, receive, loaded,
):
    me, fs = lax.axis_index("tp"), lax.axis_index("fs")
    count, fs_count = lax.axis_size("tp"), lax.axis_size("fs")
    chip, core = me // 2, me % 2
    other = 1 - chip
    sib, far, diag = chip * 2 + (1 - core), other * 2 + core, other * 2 + (1 - core)
    line = fs_count // 2
    z, y = fs // 2, fs % 2
    pair = z * 2 + (1 - y)
    z_mate = z + 1 - 2 * (z % 2)
    length, width = up.shape[1:]
    depth = down.shape[1]
    tap_count = taps_a.shape[0]
    reach = tap_count - 1
    group_count = width // GROUP
    shard = out.shape[0]
    quarter = length // 4

    def to(index):
        return {"tp": index}

    def to_fs(index):
        return {"fs": index}

    fs_others = [lax.rem(fs + by, fs_count) for by in range(1, fs_count)]
    numbers = itertools.count()
    pending = []

    def copy_of(source, target, where, send_at=None, receive_at=None):
        number = next(numbers) if send_at is None else send_at
        assert number < COPIES
        return pltpu.make_async_remote_copy(
            src_ref=source,
            dst_ref=target,
            send_sem=send.at[number],
            recv_sem=receive.at[number if receive_at is None else receive_at],
            device_id=where,
            device_id_type=MESH,
        )

    def launch(source, target, where):
        copy = copy_of(source, target, where)
        copy.start()
        pending.append(copy)
        return copy

    def rows(index):
        return span(index, length)

    def cols(index):
        return span(index, depth)

    def group(g):
        return pl.ds(g * GROUP, GROUP)

    def chunks(g, step):
        def at(i, carry):
            step(pl.ds(pl.multiple_of(g * GROUP + i * CHUNK, CHUNK), CHUNK))
            return carry

        lax.fori_loop(0, GROUP // CHUNK, at, 0)

    def depth_chunks(step, part=0, parts=1):
        per_part = depth // (CHUNK * parts)

        def at(i, carry):
            step(span(part * per_part + i, CHUNK))
            return carry

        lax.fori_loop(0, per_part, at, 0)

    sources = (
        (up_a_hbm, up.at[0]), (up_v_hbm, up.at[1]), (cot_hbm, cot), (taps_a_hbm, taps_a),
        (taps_v_hbm, taps_v), (bias_a_hbm, bias_a), (bias_v_hbm, bias_v), (down_hbm, down),
        (hidden_hbm, hidden), (w_a_hbm, weights.at[0]), (w_v_hbm, weights.at[1]),
    )
    loads = [
        pltpu.make_async_copy(source, target, loaded.at[i])
        for i, (source, target) in enumerate(sources)
    ]
    for load in loads[:7]:
        load.start()

    after[...] = jnp.zeros(after.shape, after.dtype)
    barrier = pltpu.get_barrier_semaphore()
    z_others = [lax.rem(z + by, line) * 2 + y for by in range(1, line)]
    everyone = [to(sib), to(far), to(diag)] + [to_fs(index) for index in fs_others]
    everyone += [{"tp": there, "fs": index} for index in z_others for there in (far, diag)]
    for where in everyone:
        pl.semaphore_signal(barrier, inc=1, device_id=where, device_id_type=MESH)
    pl.semaphore_wait(barrier, len(everyone))

    loads[0].wait()
    loads[1].wait()
    has_before, has_after = me > 0, me < count - 1
    last = pl.ds(length - HALO, HALO)
    halo = [copy_of(up.at[r, last, :], before.at[r], to(lax.rem(me + 1, count))) for r in range(2)]

    @pl.when(has_after)
    def _():
        for copy in halo:
            copy.start()

    @pl.when(jnp.logical_not(has_before))
    def _():
        before[...] = jnp.zeros(before.shape, before.dtype)

    loads[2].wait()
    for load in loads[3:7]:
        load.wait()
    for r, (taps, bias) in enumerate(((taps_a, bias_a), (taps_v, bias_v))):
        at = r * (tap_count + 1)
        params[at : at + tap_count, :] = taps[...].astype(F32)
        params[at + tap_count : at + tap_count + 1, :] = bias[...].astype(F32)[None, :]
    mine = span((z % 2) * 2 + y, quarter)

    def quarter_of(index):
        at = index * length + ((z % 2) * 2 + y) * quarter
        return columns.at[pl.ds(pl.multiple_of(at, quarter), quarter), :]

    cot_diag = launch(cot.at[mine, cols(diag)], quarter_of(me), to(diag))
    cot_far = launch(cot.at[mine, cols(far)], quarter_of(me), to(far))
    cot_sib = launch(cot.at[:, cols(sib)], columns.at[rows(me), :], to(sib))
    for load in loads[7:]:
        load.start()
    columns[rows(me), :] = cot[:, cols(me)]

    def share(index):
        mates = (pair, z_mate * 2 + y, z_mate * 2 + (1 - y))
        return [launch(quarter_of(index), quarter_of(index), to_fs(mate)) for mate in mates]

    def shifted(r, lanes):
        ext = jnp.concatenate([before[r, :, lanes].astype(F32), up[r, :, lanes].astype(F32)], 0)
        return [ext[HALO - reach + k : HALO - reach + k + length] for k in range(tap_count)]

    def param(r, k, lanes):
        at = r * (tap_count + 1) + k
        return params[at : at + 1, lanes]

    def forward(lanes):
        pre = []
        for r in range(2):
            taken = shifted(r, lanes)
            total = jnp.broadcast_to(param(r, tap_count, lanes), (length, CHUNK))
            for k in range(tap_count):
                total = total + param(r, k, lanes) * taken[k]
            pre.append(total)
        pre_a, pre_v = pre
        square = pre_a * pre_a
        bent = jnp.tanh(ROOT_TWO_OVER_PI * pre_a * (1.0 + CUBIC * square))
        half = 0.5 * (1.0 + bent)
        gelu = pre_a * half
        slope = half + 0.5 * pre_a * (1.0 - bent * bent) * (
            ROOT_TWO_OVER_PI * (1.0 + 3.0 * CUBIC * square)
        )
        all_m[rows(me), lanes] = (gelu * pre_v).astype(BF16)
        gated[:, lanes] = gelu
        factor[:, lanes] = pre_v * slope

    mixed_far, mixed_sib = [], []

    def spread_mixed(g):
        here = all_m.at[rows(me), group(g)]
        mixed_far.append(launch(here, here, to(far)))
        mixed_sib.append(launch(here, here, to(sib)))

    @pl.when(has_before)
    def _():
        for copy in halo:
            copy.wait_recv()

    for g in range(group_count):
        chunks(g, forward)
        spread_mixed(g)
        if g == 0:
            cot_diag.wait_recv()
            shared_diag = share(diag)
        if g == 1:
            cot_far.wait_recv()
            shared_far = share(far)

    loads[7].wait()

    def partial(index, g, finish):
        def step(lanes):
            finish(lanes, contract_last(columns[rows(index), :], down[lanes, :]))

        chunks(g, step)

    def keep(target):
        def finish(lanes, value):
            target[:, lanes] = value.astype(target.dtype)

        return finish

    def add_far(lanes, value):
        to_far[:, lanes] = (value + from_sib_far[:, lanes].astype(F32)).astype(BF16)

    for g in range(group_count):
        partial(me, g, keep(own))
    cot_sib.wait_recv()
    for g in range(group_count):
        partial(sib, g, keep(to_sib))
    near = launch(to_sib, from_sib, to(sib))
    relayed, crossed = [], []

    def diag_part(g):
        partial(diag, g, keep(to_sib_far))
        relayed.append(launch(to_sib_far.at[:, group(g)], from_sib_far.at[:, group(g)], to(sib)))

    def far_part(g):
        relayed[g].wait_recv()
        partial(far, g, add_far)
        crossed.append(launch(to_far.at[:, group(g)], from_far.at[:, group(g)], to(far)))

    for copy in shared_diag:
        copy.wait_recv()
    diag_part(0)
    for g in range(1, group_count):
        diag_part(g)
        if g == 1:
            for copy in shared_far:
                copy.wait_recv()
        far_part(g - 1)
    far_part(group_count - 1)

    mixed_relays = []

    def relay_mixed(g):
        mixed_far[g].wait_recv()
        there = all_m.at[rows(far), group(g)]
        mixed_relays.append(launch(there, there, to(sib)))

    for g in range(group_count):
        relay_mixed(g)
    for copy in mixed_sib + mixed_relays:
        copy.wait_recv()
    own_down[...] = jnp.zeros(own_down.shape, F32)

    def down_step(lanes):
        value = contract_first(columns[:, lanes], all_m[...])
        own_down[...] += jnp.sum(value * value, axis=0, keepdims=True)

    depth_chunks(down_step)
    got_down[me] = own_down[...]
    tp_others = [lax.rem(me + by, count) for by in range(1, count)]
    down_copies = [launch(own_down, got_down.at[me], to(index)) for index in tp_others]

    def combine(lanes):
        total = own[:, lanes] + from_sib[:, lanes].astype(F32) + from_far[:, lanes].astype(F32)
        grad_mixed = total.astype(BF16).astype(F32)
        for r, scale in ((0, factor), (1, gated)):
            pre_grad = grad_mixed * scale[:, lanes]
            grads[r, :, lanes] = pre_grad
            found = [
                jnp.sum(pre_grad * taken, axis=0, keepdims=True) for taken in shifted(r, lanes)
            ]
            found.append(jnp.sum(pre_grad, axis=0, keepdims=True))
            own_sums[r, :, lanes] = jnp.concatenate(found, 0)

    def backward(lanes):
        for r in range(2):
            ext = jnp.concatenate([grads[r, :, lanes], after[r, :, lanes]], 0)
            total = jnp.zeros((length, CHUNK), F32)
            for k in range(tap_count):
                total = total + param(r, k, lanes) * ext[reach - k : reach - k + length]
            all_g[r, rows(me), lanes] = total.astype(BF16)

    first = pl.ds(0, reach)
    left = lax.rem(me + count - 1, count)
    final = group_count - 1
    backs, sent_g = [], {}

    def cross(g, j):
        here = all_g.at[core, rows(chip * 2 + j), group(g)]
        sent_g[g, j] = launch(here, here, to(far))

    near.wait_recv()
    for g in range(group_count):
        crossed[g].wait_recv()
        chunks(g, combine)
        back = [
            copy_of(grads.at[r, first, group(g)], after.at[r, first, group(g)], to(left))
            for r in range(2)
        ]
        backs += back

        @pl.when(has_before)
        def _():
            for copy in back:
                copy.start()

        @pl.when(has_after)
        def _():
            for copy in back:
                copy.wait_recv()

        chunks(g, backward)
        beside = []
        for r in range(2):
            here = all_g.at[r, rows(me), group(g)]
            beside.append(launch(here, here, to(sib)))
        for copy in beside:
            copy.wait_recv()
        cross(g, 0)
        if g < final - 1:
            cross(g, 1)
    cross(final - 1, 1)
    cross(final, 1)
    side_sums = launch(own_sums.at[1 - core], sib_sums, to(sib))

    loads[9].wait()
    loads[10].wait()

    def product(at, lanes, ks):
        total = contract_last(all_g[0, at, ks], weights[0, lanes, ks])
        return total + contract_last(all_g[1, at, ks], weights[1, lanes, ks])

    both = span(chip, 2 * length)
    blocks = (me, sib, other * 2, other * 2 + 1)

    def slab(k, index):
        return pl.ds(pl.multiple_of(blocks[k] * length + index * shard, shard), shard)

    pair_copies, line_copies, last_copies = {}, {}, {}
    parts = 2 if depth % (2 * CHUNK) == 0 else 1
    whole = pl.ds(0, depth)

    def part_of(part):
        return pl.ds(part * (depth // parts), depth // parts)

    def send_pair(k, part=None):
        at = whole if part is None else part_of(part)
        for there in range(line):
            to_pair[k, there * shard : (there + 1) * shard, at] = terms[
                slab(k, there * 2 + (1 - y)), at
            ].astype(BF16)
        pair_copies[k, part] = launch(to_pair.at[k, :, at], from_pair.at[k, :, at], to_fs(pair))

    straight = {by: [next(numbers) for _ in range(2)] for by in range(line)}

    def send_line(k, part=None):
        at = whole if part is None else part_of(part)
        pair_copies[k, part].wait_recv()
        line_copies[k, part] = []
        for by in sorted(range(1, line), key=lambda by: -min(by, line - by)) + [0]:
            there = lax.rem(z + by, line)
            added = terms[slab(k, there * 2 + y), at] + from_pair[
                k, span(there, shard), at
            ].astype(F32)
            if k >= 2:
                to_line[k, by, :, at] = added.astype(BF16)
                copy = copy_of(
                    to_line.at[k, by, :, at], arrived.at[core, by, :, at],
                    {"tp": blocks[k], "fs": there * 2 + y},
                    receive_at=straight[by][0] + core,
                )
                copy.start()
                pending.append(copy)
            elif by == 0:
                kept[k, :, at] = added
            else:
                to_line[k, by, :, at] = added.astype(BF16)
                line_copies[k, part].append((by, launch(
                    to_line.at[k, by, :, at], from_line.at[k, by, :, at], to_fs(there * 2 + y)
                )))

    def settle(k):
        total = kept[k]
        for by, copy in line_copies[k, None]:
            copy.wait_recv()
            total = total + from_line[k, by].astype(F32)
        if k == 0:
            out[:, cols(me)] = total.astype(BF16)
        else:
            settled[...] = total.astype(BF16)
            last_copies[k] = launch(settled, out.at[:, cols(me)], to(sib))

    def settle_straight():
        for j in range(2):
            total = None
            for by in range(line):
                copy_of(
                    arrived.at[j, by], arrived.at[j, by], to(far), receive_at=straight[by][j]
                ).wait_recv()
                value = arrived[j, by].astype(F32)
                total = value if total is None else total + value
            out[:, cols(other * 2 + j)] = total.astype(BF16)

    def relay(*which):
        started = []
        for g, j in which:
            sent_g[g, j].wait_recv()
            there = all_g.at[core, rows(other * 2 + j), group(g)]
            started.append(launch(there, there, to(sib)))
        return started

    def arrive(started):
        for copy in started:
            copy.wait_recv()

    def add(at, g, fresh=False, part=0, split=1):
        def step(lanes):
            value = product(at, lanes, group(g))
            terms[at, lanes] = value if fresh else terms[at, lanes] + value

        depth_chunks(step, part, split)

    own_norms[...] = jnp.zeros(own_norms.shape, F32)

    def norm_group(g, roles=(0, 1)):
        def step(lanes):
            for r in roles:
                value = contract_first(all_g[r, :, lanes], hidden[...])
                own_norms[r : r + 1, :] += jnp.sum(value * value, axis=0, keepdims=True)

        chunks(g, step)

    theirs = span(other, 2 * length)
    near_block, last_block = rows(other * 2), rows(other * 2 + 1)
    started = relay((0, 0))
    depth_chunks(lambda lanes: terms.__setitem__(
        (both, lanes), product(both, lanes, pl.ds(0, width))
    ))
    send_pair(0)
    send_pair(1)
    started += relay((0, 1))
    side_sums.wait_recv()
    chip_sums[...] = own_sums[core] + sib_sums[...]
    cross_sums = launch(chip_sums, far_sums, to(far))
    loads[8].wait()
    for g in range(final - 1):
        if g > 0:
            started = relay((g, 0), (g, 1))
        arrive(started)
        add(theirs, g, g == 0)
        norm_group(g)
    started = relay((final - 1, 0))
    cross_sums.wait_recv()
    sums[core] = chip_sums[...] + far_sums[...]
    side_total = launch(sums.at[core], sums.at[core], to(sib))
    send_line(0)
    send_line(1)
    arrive(started)
    add(near_block, final - 1)
    started = relay((final, 0))
    side_total.wait_recv()
    total_sums = sums[...]
    own_squares[...] = jnp.broadcast_to(
        jnp.sum(total_sums * total_sums, axis=2, keepdims=True), own_squares.shape
    )
    got_squares[fs] = own_squares[...]
    square_copies = [launch(own_squares, got_squares.at[fs], to_fs(index)) for index in fs_others]
    arrive(started)
    add(near_block, final)
    send_pair(2)
    arrive(relay((final - 1, 1)))
    add(last_block, final - 1)
    norm_group(final - 1, (0,))
    started = relay((final, 1))
    norm_group(final - 1, (1,))
    arrive(started)
    for part in range(parts):
        add(last_block, final, False, part, parts)
        send_pair(3, part)
    send_line(2)
    norm_group(final)
    got_norms[fs] = own_norms[...]
    norm_copies = [launch(own_norms, got_norms.at[fs], to_fs(index)) for index in fs_others]
    for part in range(parts):
        send_line(3, part)
    settle(0)
    settle(1)
    for copies in (down_copies, square_copies, norm_copies):
        for copy in copies:
            copy.wait_recv()

    def gathered(ref, size):
        total = ref[0]
        for index in range(1, size):
            total = total + ref[index]
        return total

    down_norms[...] = gathered(got_down, count)
    squares[...] = gathered(got_squares, fs_count)
    norms[...] = gathered(got_norms, fs_count)
    last_copies[1].wait_recv()
    settle_straight()
    for copy in pending:
        copy.wait_send()

    @pl.when(has_after)
    def _():
        for copy in halo:
            copy.wait_send()

    @pl.when(has_before)
    def _():
        for copy in backs:
            copy.wait_send()


def gradients(
    hidden_in, up_act, up_val, cotangent, w_act, w_val, w_down,
    conv_act, conv_val, bias_act, bias_val,
):
    length, width = up_act.shape
    depth = w_down.shape[1]
    tp_count, fs_count = lax.axis_size("tp"), lax.axis_size("fs")
    positions = length * tp_count
    shard = length // fs_count
    line = fs_count // 2
    stat_rows = conv_act.shape[0] + 1
    vmem = pl.BlockSpec(memory_space=pltpu.VMEM)
    hbm = pl.BlockSpec(memory_space=pltpu.HBM)
    block = pltpu.VMEM((length, width), BF16)
    wide = pltpu.VMEM((length, width), F32)
    slots = pltpu.VMEM((4, line * shard, depth), BF16)
    pieces = pltpu.VMEM((4, line, shard, depth), BF16)
    half_sums = pltpu.VMEM((stat_rows, width), F32)
    return pl.pallas_call(
        gradient_kernel,
        out_shape=(
            jax.ShapeDtypeStruct((positions, depth), BF16),
            jax.ShapeDtypeStruct((2, positions, width), BF16),
            jax.ShapeDtypeStruct((positions, width), BF16),
            jax.ShapeDtypeStruct((2, stat_rows, width), F32),
            jax.ShapeDtypeStruct((shard, depth * tp_count), BF16),
            jax.ShapeDtypeStruct((2, depth), F32),
            jax.ShapeDtypeStruct((1, width), F32),
            jax.ShapeDtypeStruct((2, stat_rows, 128), F32),
        ),
        in_specs=[hbm] * 11,
        out_specs=(vmem,) * 8,
        scratch_shapes=[
            pltpu.VMEM(hidden_in.shape, BF16),
            pltpu.VMEM((2, length, width), BF16),
            pltpu.VMEM(cotangent.shape, BF16),
            pltpu.VMEM((2,) + w_act.shape, BF16),
            pltpu.VMEM(w_down.shape, BF16),
            pltpu.VMEM(conv_act.shape, BF16), pltpu.VMEM(conv_val.shape, BF16),
            pltpu.VMEM((width,), BF16), pltpu.VMEM((width,), BF16),
            pltpu.VMEM((2 * stat_rows, width), F32),
            pltpu.VMEM((2, HALO, width), BF16), pltpu.VMEM((2, TAIL, width), F32),
            pltpu.VMEM((2, length, width), F32), wide, wide,
            wide, block, block, block, block, block, block,
            pltpu.VMEM((positions, depth), F32),
            slots, slots, pltpu.VMEM((2, shard, depth), F32), pieces,
            pltpu.VMEM((2, line, shard, depth), BF16), pltpu.VMEM((shard, depth), BF16),
            pltpu.VMEM((2, line, shard, depth), BF16),
            pltpu.VMEM((2, stat_rows, width), F32), half_sums, half_sums, half_sums,
            pltpu.VMEM((2, depth), F32), pltpu.VMEM((fs_count, 2, depth), F32),
            pltpu.VMEM((1, width), F32), pltpu.VMEM((tp_count, 1, width), F32),
            pltpu.VMEM((2, stat_rows, 128), F32), pltpu.VMEM((fs_count, 2, stat_rows, 128), F32),
            pltpu.SemaphoreType.DMA((COPIES,)), pltpu.SemaphoreType.DMA((COPIES,)),
            pltpu.SemaphoreType.DMA((11,)),
        ],
        compiler_params=pltpu.CompilerParams(
            collective_id=0, has_side_effects=True, vmem_limit_bytes=34 * 1024 * 1024
        ),
    )(*(
        pltpu.with_memory_space_constraint(operand, pltpu.HBM)
        for operand in (
            hidden_in, up_act, up_val, cotangent, w_act, w_val, w_down,
            conv_act, conv_val, bias_act, bias_val,
        )
    ))


def kernels_fit(up_act, w_down, conv_act):
    length, width = up_act.shape
    fs_count, tp_count = lax.axis_size("fs"), lax.axis_size("tp")
    return (
        tp_count == 4
        and fs_count % 4 == 0
        and width % GROUP == 0
        and width // GROUP > 2
        and w_down.shape[1] % ROWS == 0
        and width % ROWS == 0
        and length % (16 * fs_count) == 0
        and conv_act.shape[0] - 1 <= TAIL
        and conv_act.shape[0] == 3
        and width * (3 * w_down.shape[1] + 32 * length) * 2 <= 32 * 1024 * 1024
    )


def weight_kernel(
    hidden, all_g, all_m, columns, sums, grad_in, norms, down_norms, squares,
    w_act, w_val, w_down, input_out, conv_a, conv_v, bias_a, bias_v,
    rows_a, rows_v, rows_d, conv_rows,
    blocks, held_conv, held_rows, held_a, held_v, held_d, held_rows_a, held_rows_v,
    done, small_done,
):
    taps = conv_a.shape[0]
    depth, width = hidden.shape[1], all_m.shape[1]
    for r in range(2):
        held_conv[r] = sums[r, :taps, :]
    held_a[...] = sums[0, taps, :]
    held_v[...] = sums[1, taps, :]
    held_d[...] = down_norms[0, :]
    held_rows_a[...] = norms[0, :]
    held_rows_v[...] = norms[1, :]
    lane = lax.broadcasted_iota(jnp.int32, (1, 128), 1)
    for r in range(2):
        row = jnp.zeros((1, 128), F32)
        for k in range(taps):
            row = jnp.where(lane == k, squares[r, k : k + 1, :], row)
        held_rows[r : r + 1, :] = row[:, :taps]
    pairs = (
        (grad_in, input_out), (held_conv.at[0], conv_a), (held_conv.at[1], conv_v),
        (held_a, bias_a), (held_v, bias_v), (held_rows_a, rows_a),
        (held_rows_v, rows_v), (held_d, rows_d), (held_rows, conv_rows),
    )
    flying = [
        pltpu.make_async_copy(source, target, small_done.at[i])
        for i, (source, target) in enumerate(pairs)
    ]
    for copy in flying:
        copy.start()
    jobs = [(hidden, all_g.at[0], w_act, at) for at in range(0, depth, ROWS)]
    jobs += [(hidden, all_g.at[1], w_val, at) for at in range(0, depth, ROWS)]
    jobs += [(all_m, columns, w_down, at) for at in range(0, width, ROWS)]
    stored = []
    for number, (left, right, target, at) in enumerate(jobs):
        slot = number % SLOTS
        if number >= SLOTS:
            stored[number - SLOTS].wait()
        size = right.shape[1]
        blocks[slot, :, :size] = contract_first(left[:, at : at + ROWS], right[...])
        stored.append(pltpu.make_async_copy(
            blocks.at[slot, :, pl.ds(0, size)], target.at[pl.ds(at, ROWS), :], done.at[slot]
        ))
        stored[number].start()
    for copy in stored[-SLOTS:] + flying:
        copy.wait()


def weight_gradients(hidden_in, all_g, all_m, columns, sums, grad_in, norms, down_norms, squares):
    depth, width = hidden_in.shape[1], all_m.shape[1]
    taps = sums.shape[1] - 1
    operands = (hidden_in, all_g, all_m, columns, sums, grad_in, norms, down_norms, squares)
    shapes = (
        (depth, width), (depth, width), (width, depth), None, (taps, width), (taps, width),
        (width,), (width,), (depth,), (depth,), (width,), (2, taps),
    )
    return pl.pallas_call(
        weight_kernel,
        out_shape=tuple(
            jax.ShapeDtypeStruct(grad_in.shape, BF16) if shape is None
            else jax.ShapeDtypeStruct(shape, F32)
            for shape in shapes
        ),
        in_specs=[pl.BlockSpec(memory_space=pltpu.VMEM)] * len(operands),
        out_specs=(pl.BlockSpec(memory_space=pltpu.HBM),) * len(shapes),
        scratch_shapes=[
            pltpu.VMEM((SLOTS, ROWS, max(depth, width)), F32),
            pltpu.VMEM((2, taps, width), F32), pltpu.VMEM((2, taps), F32),
            pltpu.VMEM((width,), F32), pltpu.VMEM((width,), F32), pltpu.VMEM((width,), F32),
            pltpu.VMEM((depth,), F32), pltpu.VMEM((depth,), F32),
            pltpu.SemaphoreType.DMA((SLOTS,)), pltpu.SemaphoreType.DMA((9,)),
        ],
        compiler_params=pltpu.CompilerParams(vmem_limit_bytes=24 * 1024 * 1024),
    )(*operands)


def with_kernels(
    hidden_in, up_act, up_val, cotangent, w_act, w_val, w_down,
    conv_act, conv_val, bias_act, bias_val,
):
    columns, all_g, all_m, sums, grad_in, norms, down_norms, squares = gradients(
        hidden_in, up_act, up_val, cotangent, w_act, w_val, w_down,
        conv_act, conv_val, bias_act, bias_val,
    )
    (
        grad_w_act, grad_w_val, grad_w_down, grad_input, conv_a, conv_v, bias_a, bias_v,
        rows_a, rows_v, rows_d, conv_rows,
    ) = weight_gradients(
        hidden_in, all_g, all_m, columns, sums, grad_in, norms, down_norms, squares
    )
    return (
        grad_input, grad_w_act, grad_w_val, grad_w_down, conv_a, conv_v,
        bias_a, bias_v, rows_a, rows_v, rows_d, conv_rows,
    )


def passed_along(value, axis, by):
    length = lax.axis_size(axis)
    pairs = [(i, i + by) for i in range(length) if 0 <= i + by < length]
    return lax.ppermute(value, axis, pairs)


def contract_last(left, right):
    return lax.dot_general(
        left, right, (((1,), (1,)), ((), ())), preferred_element_type=jnp.float32
    )


def contract_first(left, right):
    return lax.dot_general(
        left, right, (((0,), (0,)), ((), ())), preferred_element_type=jnp.float32
    )


def conv_ahead(extended, taps, bias, length):
    total = jnp.zeros((length, extended.shape[1]), jnp.float32) + bias.astype(jnp.float32)
    for offset in range(taps.shape[0]):
        total = total + taps[offset].astype(jnp.float32) * extended[offset : offset + length]
    return total


def conv_behind(extended, taps, length):
    reach = taps.shape[0] - 1
    total = jnp.zeros((length, extended.shape[1]), jnp.float32)
    for offset in range(taps.shape[0]):
        total = (
            total
            + taps[offset].astype(jnp.float32) * extended[reach - offset : reach - offset + length]
        )
    return total.astype(jnp.bfloat16)


def tap_grads(grad_pre, extended, tap_count):
    length = grad_pre.shape[0]
    rows = [
        jnp.sum(grad_pre * extended[offset : offset + length], axis=0)
        for offset in range(tap_count)
    ]
    return (jnp.stack(rows, 0), jnp.sum(grad_pre, axis=0))


def per_device(
    hidden_in,
    up_act,
    up_val,
    cotangent,
    w_act,
    w_val,
    w_down,
    conv_act,
    conv_val,
    bias_act,
    bias_val,
):
    if kernels_fit(up_act, w_down, conv_act):
        return with_kernels(
            hidden_in, up_act, up_val, cotangent, w_act, w_val, w_down,
            conv_act, conv_val, bias_act, bias_val,
        )
    local_rows = cotangent.shape[0]
    tap_count = conv_act.shape[0]
    reach = tap_count - 1
    tp_count = lax.axis_size("tp")
    fs_count = lax.axis_size("fs")
    down_whole = lax.all_gather(w_down, "tp", axis=1, tiled=True)
    prev_act, prev_val = passed_along(
        (up_act[local_rows - reach :], up_val[local_rows - reach :]), "tp", 1
    )
    ext_act = jnp.concatenate([prev_act, up_act], 0).astype(jnp.float32)
    ext_val = jnp.concatenate([prev_val, up_val], 0).astype(jnp.float32)
    pre_act = conv_ahead(ext_act, conv_act, bias_act, local_rows)
    pre_val = conv_ahead(ext_val, conv_val, bias_val, local_rows)
    gelu_act, gelu_back = jax.vjp(jax.nn.gelu, pre_act)
    mixed = (gelu_act * pre_val).astype(jnp.bfloat16)
    grad_mixed = contract_last(cotangent, down_whole).astype(jnp.bfloat16)
    grad_mixed = lax.optimization_barrier(grad_mixed).astype(jnp.float32)
    grad_pre_act = gelu_back(grad_mixed * pre_val)[0]
    grad_pre_val = grad_mixed * gelu_act
    next_act, next_val = passed_along((grad_pre_act[:reach], grad_pre_val[:reach]), "tp", -1)
    grad_up_act = conv_behind(jnp.concatenate([grad_pre_act, next_act], 0), conv_act, local_rows)
    grad_up_val = conv_behind(jnp.concatenate([grad_pre_val, next_val], 0), conv_val, local_rows)
    taps_act, sums_act = tap_grads(grad_pre_act, ext_act, tap_count)
    taps_val, sums_val = tap_grads(grad_pre_val, ext_val, tap_count)
    all_up_act, all_up_val, all_mixed = (
        lax.all_gather(grad_up_act, "tp", axis=0, tiled=True),
        lax.all_gather(grad_up_val, "tp", axis=0, tiled=True),
        lax.all_gather(mixed, "tp", axis=0, tiled=True),
    )
    cot_columns = lax.all_to_all(cotangent, "tp", split_axis=1, concat_axis=0, tiled=True)
    grad_w_act = contract_first(hidden_in, all_up_act)
    grad_w_val = contract_first(hidden_in, all_up_val)
    grad_w_down = contract_first(all_mixed, cot_columns)
    shard_rows = local_rows // fs_count
    block_rows = tp_count * shard_rows

    def select_rows(gathered):
        shaped = gathered.reshape(tp_count, fs_count, shard_rows, gathered.shape[1])
        return jnp.transpose(shaped, (1, 0, 2, 3)).reshape(
            lax.axis_size("fs") * block_rows, gathered.shape[1]
        )

    summed = lax.psum_scatter(
        contract_last(select_rows(all_up_act), w_act)
        + contract_last(select_rows(all_up_val), w_val),
        "fs",
        scatter_dimension=0,
        tiled=True,
    ).astype(jnp.bfloat16)
    grad_input = lax.all_to_all(summed, "tp", split_axis=0, concat_axis=1, tiled=True)
    down_squares = jnp.sum(grad_w_down * grad_w_down, axis=1)
    taps_act, taps_val, sums_act, sums_val, rows_down = lax.psum(
        (taps_act, taps_val, sums_act, sums_val, down_squares), "tp"
    )
    tap_squares = jnp.stack(
        [jnp.sum(taps_act * taps_act, axis=1), jnp.sum(taps_val * taps_val, axis=1)], 0
    )
    rows_act, rows_val, conv_rows = lax.psum(
        (
            jnp.sum(grad_w_act * grad_w_act, axis=1),
            jnp.sum(grad_w_val * grad_w_val, axis=1),
            tap_squares,
        ),
        "fs",
    )
    return (
        grad_input,
        grad_w_act,
        grad_w_val,
        grad_w_down,
        taps_act,
        taps_val,
        sums_act,
        sums_val,
        rows_act,
        rows_val,
        rows_down,
        conv_rows,
    )


def solution(mesh):
    return jax.shard_map(
        per_device,
        mesh=mesh,
        in_specs=(
            P(None, "tp"),
            P("tp", "fs"),
            P("tp", "fs"),
            P("tp", None),
            P("tp", "fs"),
            P("tp", "fs"),
            P("fs", "tp"),
            P(None, "fs"),
            P(None, "fs"),
            P("fs"),
            P("fs"),
        ),
        out_specs=(
            P(("tp", "fs"), None),
            P("tp", "fs"),
            P("tp", "fs"),
            P("fs", "tp"),
            P(None, "fs"),
            P(None, "fs"),
            P("fs"),
            P("fs"),
            P("tp"),
            P("tp"),
            P("fs"),
            P(),
        ),
        check_vma=False,
    )
```

```python
import itertools

import jax
import jax.numpy as jnp
from jax import lax
from jax.experimental import pallas as pl
from jax.experimental.pallas import tpu as pltpu
from jax.sharding import PartitionSpec as P

MESH = pl.DeviceIdType.MESH
F32 = jnp.float32
BF16 = jnp.bfloat16
CHUNK = 256
GROUP = 512
HALO = 8
TAIL = 8
COPIES = 144
ROWS = 512
SLOTS = 3
PARTS = 2
ROOT_TWO_OVER_PI = 0.7978845608028654
CUBIC = 0.044715


def span(index, size):
    return pl.ds(pl.multiple_of(index * size, size), size)


def gradient_kernel(
    hidden_hbm, up_a_hbm, up_v_hbm, cot_hbm, w_a_hbm, w_v_hbm, down_hbm,
    taps_a_hbm, taps_v_hbm, bias_a_hbm, bias_v_hbm,
    grad_down, all_g, sums, out, norms, down_norms, squares,
    columns, all_m, hidden, up, cot, weights, down, taps_a, taps_v, bias_a, bias_v, params,
    before, after, grads, gated, factor,
    own, to_sib, from_sib, to_sib_far, from_sib_far, to_far, from_far,
    terms, to_pair, from_pair, kept, to_line, from_line, settled, arrived,
    own_sums, sib_sums, chip_sums, far_sums, own_norms, got_norms, own_down, got_down,
    own_squares, got_squares,
    send, receive, loaded,
):
    me, fs = lax.axis_index("tp"), lax.axis_index("fs")
    count, fs_count = lax.axis_size("tp"), lax.axis_size("fs")
    chip, core = me // 2, me % 2
    other = 1 - chip
    sib, far, diag = chip * 2 + (1 - core), other * 2 + core, other * 2 + (1 - core)
    line = fs_count // 2
    z, y = fs // 2, fs % 2
    pair = z * 2 + (1 - y)
    z_mate = z + 1 - 2 * (z % 2)
    length, width = up.shape[1:]
    depth = down.shape[1]
    tap_count = taps_a.shape[0]
    reach = tap_count - 1
    group_count = width // GROUP
    shard = out.shape[0]
    quarter = length // 4

    def to(index):
        return {"tp": index}

    def to_fs(index):
        return {"fs": index}

    fs_others = [lax.rem(fs + by, fs_count) for by in range(1, fs_count)]
    numbers = itertools.count()
    pending = []

    def copy_of(source, target, where, send_at=None, receive_at=None):
        number = next(numbers) if send_at is None else send_at
        assert number < COPIES
        return pltpu.make_async_remote_copy(
            src_ref=source,
            dst_ref=target,
            send_sem=send.at[number],
            recv_sem=receive.at[number if receive_at is None else receive_at],
            device_id=where,
            device_id_type=MESH,
        )

    def launch(source, target, where):
        copy = copy_of(source, target, where)
        copy.start()
        pending.append(copy)
        return copy

    def rows(index):
        return span(index, length)

    def cols(index):
        return span(index, depth)

    def group(g):
        return pl.ds(g * GROUP, GROUP)

    def chunks(g, step):
        def at(i, carry):
            step(pl.ds(pl.multiple_of(g * GROUP + i * CHUNK, CHUNK), CHUNK))
            return carry

        lax.fori_loop(0, GROUP // CHUNK, at, 0)

    def depth_chunks(step, part=0, parts=1):
        per_part = depth // (CHUNK * parts)

        def at(i, carry):
            step(span(part * per_part + i, CHUNK))
            return carry

        lax.fori_loop(0, per_part, at, 0)

    sources = (
        (up_a_hbm, up.at[0]), (up_v_hbm, up.at[1]), (cot_hbm, cot), (taps_a_hbm, taps_a),
        (taps_v_hbm, taps_v), (bias_a_hbm, bias_a), (bias_v_hbm, bias_v), (down_hbm, down),
        (hidden_hbm, hidden), (w_a_hbm, weights.at[0]), (w_v_hbm, weights.at[1]),
    )
    loads = [
        pltpu.make_async_copy(source, target, loaded.at[i])
        for i, (source, target) in enumerate(sources)
    ]
    for load in loads[:7]:
        load.start()

    after[...] = jnp.zeros(after.shape, after.dtype)
    barrier = pltpu.get_barrier_semaphore()
    z_others = [lax.rem(z + by, line) * 2 + y for by in range(1, line)]
    everyone = [to(sib), to(far), to(diag)] + [to_fs(index) for index in fs_others]
    everyone += [{"tp": there, "fs": index} for index in z_others for there in (far, diag)]
    for where in everyone:
        pl.semaphore_signal(barrier, inc=1, device_id=where, device_id_type=MESH)
    pl.semaphore_wait(barrier, len(everyone))

    loads[0].wait()
    loads[1].wait()
    has_before, has_after = me > 0, me < count - 1
    last = pl.ds(length - HALO, HALO)
    halo = [copy_of(up.at[r, last, :], before.at[r], to(lax.rem(me + 1, count))) for r in range(2)]

    @pl.when(has_after)
    def _():
        for copy in halo:
            copy.start()

    @pl.when(jnp.logical_not(has_before))
    def _():
        before[...] = jnp.zeros(before.shape, before.dtype)

    loads[2].wait()
    for load in loads[3:7]:
        load.wait()
    for r, (taps, bias) in enumerate(((taps_a, bias_a), (taps_v, bias_v))):
        at = r * (tap_count + 1)
        params[at : at + tap_count, :] = taps[...].astype(F32)
        params[at + tap_count : at + tap_count + 1, :] = bias[...].astype(F32)[None, :]
    mine = span((z % 2) * 2 + y, quarter)

    def quarter_of(index):
        at = index * length + ((z % 2) * 2 + y) * quarter
        return columns.at[pl.ds(pl.multiple_of(at, quarter), quarter), :]

    cot_diag = launch(cot.at[mine, cols(diag)], quarter_of(me), to(diag))
    cot_far = launch(cot.at[mine, cols(far)], quarter_of(me), to(far))
    cot_sib = launch(cot.at[:, cols(sib)], columns.at[rows(me), :], to(sib))
    for load in loads[7:]:
        load.start()
    columns[rows(me), :] = cot[:, cols(me)]

    def share(index):
        mates = (pair, z_mate * 2 + y, z_mate * 2 + (1 - y))
        return [launch(quarter_of(index), quarter_of(index), to_fs(mate)) for mate in mates]

    def shifted(r, lanes):
        ext = jnp.concatenate([before[r, :, lanes].astype(F32), up[r, :, lanes].astype(F32)], 0)
        return [ext[HALO - reach + k : HALO - reach + k + length] for k in range(tap_count)]

    def param(r, k, lanes):
        at = r * (tap_count + 1) + k
        return params[at : at + 1, lanes]

    def forward(lanes):
        pre = []
        for r in range(2):
            taken = shifted(r, lanes)
            total = jnp.broadcast_to(param(r, tap_count, lanes), (length, CHUNK))
            for k in range(tap_count):
                total = total + param(r, k, lanes) * taken[k]
            pre.append(total)
        pre_a, pre_v = pre
        square = pre_a * pre_a
        bent = jnp.tanh(ROOT_TWO_OVER_PI * pre_a * (1.0 + CUBIC * square))
        half = 0.5 * (1.0 + bent)
        gelu = pre_a * half
        slope = half + 0.5 * pre_a * (1.0 - bent * bent) * (
            ROOT_TWO_OVER_PI * (1.0 + 3.0 * CUBIC * square)
        )
        all_m[rows(me), lanes] = (gelu * pre_v).astype(BF16)
        gated[:, lanes] = gelu
        factor[:, lanes] = pre_v * slope

    mixed_far, mixed_sib = [], []

    def spread_mixed(g):
        here = all_m.at[rows(me), group(g)]
        mixed_far.append(launch(here, here, to(far)))
        mixed_sib.append(launch(here, here, to(sib)))

    @pl.when(has_before)
    def _():
        for copy in halo:
            copy.wait_recv()

    for g in range(group_count):
        chunks(g, forward)
        spread_mixed(g)
        if g == 0:
            cot_diag.wait_recv()
            shared_diag = share(diag)
        if g == 1:
            cot_far.wait_recv()
            shared_far = share(far)

    loads[7].wait()

    def partial(index, g, finish):
        def step(lanes):
            finish(lanes, contract_last(columns[rows(index), :], down[lanes, :]))

        chunks(g, step)

    def keep(target):
        def finish(lanes, value):
            target[:, lanes] = value.astype(target.dtype)

        return finish

    def add_far(lanes, value):
        to_far[:, lanes] = (value + from_sib_far[:, lanes].astype(F32)).astype(BF16)

    for g in range(group_count):
        partial(me, g, keep(own))
    cot_sib.wait_recv()
    for g in range(group_count):
        partial(sib, g, keep(to_sib))
    near = launch(to_sib, from_sib, to(sib))
    relayed, crossed = [], []

    def diag_part(g):
        partial(diag, g, keep(to_sib_far))
        relayed.append(launch(to_sib_far.at[:, group(g)], from_sib_far.at[:, group(g)], to(sib)))

    def far_part(g):
        relayed[g].wait_recv()
        partial(far, g, add_far)
        crossed.append(launch(to_far.at[:, group(g)], from_far.at[:, group(g)], to(far)))

    for copy in shared_diag:
        copy.wait_recv()
    diag_part(0)
    for g in range(1, group_count):
        diag_part(g)
        if g == 1:
            for copy in shared_far:
                copy.wait_recv()
        far_part(g - 1)
    far_part(group_count - 1)

    mixed_relays = []

    def relay_mixed(g):
        mixed_far[g].wait_recv()
        there = all_m.at[rows(far), group(g)]
        mixed_relays.append(launch(there, there, to(sib)))

    for g in range(group_count):
        relay_mixed(g)

    def down_step(lanes):
        value = contract_first(all_m[:, lanes], columns[...])
        grad_down[lanes, :] = value
        square = value * value
        folded = square[:, :128]
        for at in range(128, depth, 128):
            folded = folded + square[:, at : at + 128]
        own_down[:, lanes] = jnp.sum(folded.T, axis=0, keepdims=True)

    for copy in mixed_sib + mixed_relays:
        copy.wait_recv()
    chunks(0, down_step)

    def combine(lanes):
        total = own[:, lanes] + from_sib[:, lanes].astype(F32) + from_far[:, lanes].astype(F32)
        grad_mixed = total.astype(BF16).astype(F32)
        for r, scale in ((0, factor), (1, gated)):
            pre_grad = grad_mixed * scale[:, lanes]
            grads[r, :, lanes] = pre_grad
            found = [
                jnp.sum(pre_grad * taken, axis=0, keepdims=True) for taken in shifted(r, lanes)
            ]
            found.append(jnp.sum(pre_grad, axis=0, keepdims=True))
            own_sums[r, :, lanes] = jnp.concatenate(found, 0)

    def backward(lanes):
        for r in range(2):
            ext = jnp.concatenate([grads[r, :, lanes], after[r, :, lanes]], 0)
            total = jnp.zeros((length, CHUNK), F32)
            for k in range(tap_count):
                total = total + param(r, k, lanes) * ext[reach - k : reach - k + length]
            all_g[r, rows(me), lanes] = total.astype(BF16)

    first = pl.ds(0, reach)
    left = lax.rem(me + count - 1, count)
    final = group_count - 1
    backs, sent_g = [], {}

    def cross(g, j, block):
        here = all_g.at[core, rows(block), group(g)]
        sent_g[g, j] = launch(here, here, to(far))

    near.wait_recv()
    for g in range(group_count):
        crossed[g].wait_recv()
        chunks(g, combine)
        back = [
            copy_of(grads.at[r, first, group(g)], after.at[r, first, group(g)], to(left))
            for r in range(2)
        ]
        backs += back

        @pl.when(has_before)
        def _():
            for copy in back:
                copy.start()

        @pl.when(has_after)
        def _():
            for copy in back:
                copy.wait_recv()

        chunks(g, backward)
        beside = []
        for r in range(2):
            here = all_g.at[r, rows(me), group(g)]
            beside.append(launch(here, here, to(sib)))
        for copy in beside:
            copy.wait_recv()
        if g < final - 1:
            cross(g, 0, me)
            cross(g, 1, sib)
        else:
            cross(g, 0, chip * 2)
    cross(final - 1, 1, chip * 2 + 1)
    cross(final, 1, chip * 2 + 1)
    side_sums = launch(own_sums.at[1 - core], sib_sums, to(sib))

    loads[9].wait()
    loads[10].wait()

    def product(at, lanes, ks):
        total = contract_last(all_g[0, at, ks], weights[0, lanes, ks])
        return total + contract_last(all_g[1, at, ks], weights[1, lanes, ks])

    both = span(chip, 2 * length)
    blocks = (me, sib, other * 2, other * 2 + 1)

    def slab(k, index):
        return pl.ds(pl.multiple_of(blocks[k] * length + index * shard, shard), shard)

    pair_copies, line_copies, last_copies = {}, {}, {}
    parts = PARTS if depth % (PARTS * CHUNK) == 0 else 1
    whole = pl.ds(0, depth)

    def part_of(part):
        return pl.ds(part * (depth // parts), depth // parts)

    def send_pair(k, part=None):
        at = whole if part is None else part_of(part)
        for there in range(line):
            to_pair[k, there * shard : (there + 1) * shard, at] = terms[
                slab(k, there * 2 + (1 - y)), at
            ].astype(BF16)
        pair_copies[k, part] = launch(to_pair.at[k, :, at], from_pair.at[k, :, at], to_fs(pair))

    straight = {by: [next(numbers) for _ in range(2)] for by in range(line)}

    def send_line(k, part=None):
        at = whole if part is None else part_of(part)
        pair_copies[k, part].wait_recv()
        line_copies[k, part] = []
        for by in sorted(range(1, line), key=lambda by: -min(by, line - by)) + [0]:
            there = lax.rem(z + by, line)
            added = terms[slab(k, there * 2 + y), at] + from_pair[
                k, span(there, shard), at
            ].astype(F32)
            if k >= 2:
                to_line[k, by, :, at] = added.astype(BF16)
                copy = copy_of(
                    to_line.at[k, by, :, at], arrived.at[core, by, :, at],
                    {"tp": blocks[k], "fs": there * 2 + y},
                    receive_at=straight[by][0] + core,
                )
                copy.start()
                pending.append(copy)
            elif by == 0:
                kept[k, :, at] = added
            else:
                to_line[k, by, :, at] = added.astype(BF16)
                line_copies[k, part].append((by, launch(
                    to_line.at[k, by, :, at], from_line.at[k, by, :, at], to_fs(there * 2 + y)
                )))

    def settle(k):
        total = kept[k]
        for by, copy in line_copies[k, None]:
            copy.wait_recv()
            total = total + from_line[k, by].astype(F32)
        if k == 0:
            out[:, cols(me)] = total.astype(BF16)
        else:
            settled[...] = total.astype(BF16)
            last_copies[k] = launch(settled, out.at[:, cols(me)], to(sib))

    def settle_straight():
        for j in range(2):
            total = None
            for by in range(line):
                copy_of(
                    arrived.at[j, by], arrived.at[j, by], to(far), receive_at=straight[by][j]
                ).wait_recv()
                value = arrived[j, by].astype(F32)
                total = value if total is None else total + value
            out[:, cols(other * 2 + j)] = total.astype(BF16)

    def relay(*which):
        started = []
        for g, j in which:
            sent_g[g, j].wait_recv()
            block = (far, diag)[j] if g < final - 1 else other * 2 + j
            there = all_g.at[core, rows(block), group(g)]
            started.append(launch(there, there, to(sib)))
        return started

    def arrive(started):
        for copy in started:
            copy.wait_recv()

    def add(at, g, fresh=False, part=0, split=1):
        def step(lanes):
            value = product(at, lanes, group(g))
            terms[at, lanes] = value if fresh else terms[at, lanes] + value

        depth_chunks(step, part, split)

    own_norms[...] = jnp.zeros(own_norms.shape, F32)

    def norm_group(g, roles=(0, 1)):
        def step(lanes):
            for r in roles:
                value = contract_first(all_g[r, :, lanes], hidden[...])
                own_norms[r : r + 1, :] += jnp.sum(value * value, axis=0, keepdims=True)

        chunks(g, step)

    theirs = span(other, 2 * length)
    near_block, last_block = rows(other * 2), rows(other * 2 + 1)
    started = relay((0, 0))
    depth_chunks(lambda lanes: terms.__setitem__(
        (both, lanes), product(both, lanes, pl.ds(0, width))
    ))
    send_pair(0)
    send_pair(1)
    started += relay((0, 1))
    for g in range(1, group_count):
        chunks(g, down_step)
    got_down[me] = own_down[...]
    tp_others = [lax.rem(me + by, count) for by in range(1, count)]
    down_copies = [launch(own_down, got_down.at[me], to(index)) for index in tp_others]
    side_sums.wait_recv()
    chip_sums[...] = own_sums[core] + sib_sums[...]
    cross_sums = launch(chip_sums, far_sums, to(far))
    loads[8].wait()
    for g in range(final - 1):
        if g > 0:
            started = relay((g, 0), (g, 1))
        arrive(started)
        add(theirs, g, g == 0)
        norm_group(g)
    started = relay((final - 1, 0))
    cross_sums.wait_recv()
    sums[core] = chip_sums[...] + far_sums[...]
    side_total = launch(sums.at[core], sums.at[core], to(sib))
    send_line(0)
    send_line(1)
    arrive(started)
    add(near_block, final - 1)
    started = relay((final, 0))
    side_total.wait_recv()
    total_sums = sums[...]
    own_squares[...] = jnp.broadcast_to(
        jnp.sum(total_sums * total_sums, axis=2, keepdims=True), own_squares.shape
    )
    got_squares[fs] = own_squares[...]
    square_copies = [launch(own_squares, got_squares.at[fs], to_fs(index)) for index in fs_others]
    arrive(started)
    add(near_block, final)
    send_pair(2)
    arrive(relay((final - 1, 1)))
    add(last_block, final - 1)
    norm_group(final - 1, (0,))
    started = relay((final, 1))
    norm_group(final - 1, (1,))
    arrive(started)
    for part in range(parts):
        add(last_block, final, False, part, parts)
        send_pair(3, part)
    send_line(2)
    norm_group(final)
    settle(0)
    settle(1)
    for part in range(parts):
        send_line(3, part)
    got_norms[fs] = own_norms[...]
    norm_copies = [launch(own_norms, got_norms.at[fs], to_fs(index)) for index in fs_others]
    for copies in (down_copies, square_copies, norm_copies):
        for copy in copies:
            copy.wait_recv()

    def gathered(ref, size):
        total = ref[0]
        for index in range(1, size):
            total = total + ref[index]
        return total

    down_norms[...] = gathered(got_down, count)
    squares[...] = gathered(got_squares, fs_count)
    norms[...] = gathered(got_norms, fs_count)
    last_copies[1].wait_recv()
    settle_straight()
    for copy in pending:
        copy.wait_send()

    @pl.when(has_after)
    def _():
        for copy in halo:
            copy.wait_send()

    @pl.when(has_before)
    def _():
        for copy in backs:
            copy.wait_send()


def gradients(
    hidden_in, up_act, up_val, cotangent, w_act, w_val, w_down,
    conv_act, conv_val, bias_act, bias_val,
):
    length, width = up_act.shape
    depth = w_down.shape[1]
    tp_count, fs_count = lax.axis_size("tp"), lax.axis_size("fs")
    positions = length * tp_count
    shard = length // fs_count
    line = fs_count // 2
    stat_rows = conv_act.shape[0] + 1
    vmem = pl.BlockSpec(memory_space=pltpu.VMEM)
    hbm = pl.BlockSpec(memory_space=pltpu.HBM)
    block = pltpu.VMEM((length, width), BF16)
    wide = pltpu.VMEM((length, width), F32)
    slots = pltpu.VMEM((4, line * shard, depth), BF16)
    pieces = pltpu.VMEM((4, line, shard, depth), BF16)
    half_sums = pltpu.VMEM((stat_rows, width), F32)
    return pl.pallas_call(
        gradient_kernel,
        out_shape=(
            jax.ShapeDtypeStruct((width, depth), F32),
            jax.ShapeDtypeStruct((2, positions, width), BF16),
            jax.ShapeDtypeStruct((2, stat_rows, width), F32),
            jax.ShapeDtypeStruct((shard, depth * tp_count), BF16),
            jax.ShapeDtypeStruct((2, depth), F32),
            jax.ShapeDtypeStruct((1, width), F32),
            jax.ShapeDtypeStruct((2, stat_rows, 128), F32),
        ),
        in_specs=[hbm] * 11,
        out_specs=(vmem,) * 7,
        scratch_shapes=[
            pltpu.VMEM((positions, depth), BF16), pltpu.VMEM((positions, width), BF16),
            pltpu.VMEM(hidden_in.shape, BF16),
            pltpu.VMEM((2, length, width), BF16),
            pltpu.VMEM(cotangent.shape, BF16),
            pltpu.VMEM((2,) + w_act.shape, BF16),
            pltpu.VMEM(w_down.shape, BF16),
            pltpu.VMEM(conv_act.shape, BF16), pltpu.VMEM(conv_val.shape, BF16),
            pltpu.VMEM((width,), BF16), pltpu.VMEM((width,), BF16),
            pltpu.VMEM((2 * stat_rows, width), F32),
            pltpu.VMEM((2, HALO, width), BF16), pltpu.VMEM((2, TAIL, width), F32),
            pltpu.VMEM((2, length, width), F32), wide, wide,
            wide, block, block, block, block, block, block,
            pltpu.VMEM((positions, depth), F32),
            slots, slots, pltpu.VMEM((2, shard, depth), F32), pieces,
            pltpu.VMEM((2, line, shard, depth), BF16), pltpu.VMEM((shard, depth), BF16),
            pltpu.VMEM((2, line, shard, depth), BF16),
            pltpu.VMEM((2, stat_rows, width), F32), half_sums, half_sums, half_sums,
            pltpu.VMEM((2, depth), F32), pltpu.VMEM((fs_count, 2, depth), F32),
            pltpu.VMEM((1, width), F32), pltpu.VMEM((tp_count, 1, width), F32),
            pltpu.VMEM((2, stat_rows, 128), F32), pltpu.VMEM((fs_count, 2, stat_rows, 128), F32),
            pltpu.SemaphoreType.DMA((COPIES,)), pltpu.SemaphoreType.DMA((COPIES,)),
            pltpu.SemaphoreType.DMA((11,)),
        ],
        compiler_params=pltpu.CompilerParams(
            collective_id=0, has_side_effects=True, vmem_limit_bytes=34 * 1024 * 1024
        ),
    )(*(
        pltpu.with_memory_space_constraint(operand, pltpu.HBM)
        for operand in (
            hidden_in, up_act, up_val, cotangent, w_act, w_val, w_down,
            conv_act, conv_val, bias_act, bias_val,
        )
    ))


def kernels_fit(up_act, w_down, conv_act):
    length, width = up_act.shape
    fs_count, tp_count = lax.axis_size("fs"), lax.axis_size("tp")
    return (
        tp_count == 4
        and fs_count % 4 == 0
        and width % GROUP == 0
        and width // GROUP > 2
        and w_down.shape[1] % ROWS == 0
        and width % ROWS == 0
        and length % (16 * fs_count) == 0
        and conv_act.shape[0] - 1 <= TAIL
        and conv_act.shape[0] == 3
        and width * (3 * w_down.shape[1] + 32 * length) * 2 <= 32 * 1024 * 1024
    )


def weight_kernel(
    hidden, all_g, grad_down, sums, grad_in, norms, down_norms, squares,
    w_act, w_val, w_down, input_out, conv_a, conv_v, bias_a, bias_v,
    rows_a, rows_v, rows_d, conv_rows,
    blocks, held_conv, held_rows, held_a, held_v, held_d, held_rows_a, held_rows_v,
    done, small_done,
):
    taps = conv_a.shape[0]
    depth = hidden.shape[1]
    down_copy = pltpu.make_async_copy(grad_down, w_down, small_done.at[9])
    down_copy.start()
    for r in range(2):
        held_conv[r] = sums[r, :taps, :]
    held_a[...] = sums[0, taps, :]
    held_v[...] = sums[1, taps, :]
    held_d[...] = down_norms[0, :]
    held_rows_a[...] = norms[0, :]
    held_rows_v[...] = norms[1, :]
    lane = lax.broadcasted_iota(jnp.int32, (1, 128), 1)
    for r in range(2):
        row = jnp.zeros((1, 128), F32)
        for k in range(taps):
            row = jnp.where(lane == k, squares[r, k : k + 1, :], row)
        held_rows[r : r + 1, :] = row[:, :taps]
    pairs = (
        (grad_in, input_out), (held_conv.at[0], conv_a), (held_conv.at[1], conv_v),
        (held_a, bias_a), (held_v, bias_v), (held_rows_a, rows_a),
        (held_rows_v, rows_v), (held_d, rows_d), (held_rows, conv_rows),
    )
    flying = [
        pltpu.make_async_copy(source, target, small_done.at[i])
        for i, (source, target) in enumerate(pairs)
    ]
    for copy in flying:
        copy.start()
    jobs = [(hidden, all_g.at[0], w_act, at) for at in range(0, depth, ROWS)]
    jobs += [(hidden, all_g.at[1], w_val, at) for at in range(0, depth, ROWS)]
    stored = []
    for number, (left, right, target, at) in enumerate(jobs):
        slot = number % SLOTS
        if number >= SLOTS:
            stored[number - SLOTS].wait()
        size = right.shape[1]
        blocks[slot, :, :size] = contract_first(left[:, at : at + ROWS], right[...])
        stored.append(pltpu.make_async_copy(
            blocks.at[slot, :, pl.ds(0, size)], target.at[pl.ds(at, ROWS), :], done.at[slot]
        ))
        stored[number].start()
    for copy in stored[-SLOTS:] + flying + [down_copy]:
        copy.wait()


def weight_gradients(hidden_in, all_g, grad_down, sums, grad_in, norms, down_norms, squares):
    width, depth = grad_down.shape
    taps = sums.shape[1] - 1
    operands = (hidden_in, all_g, grad_down, sums, grad_in, norms, down_norms, squares)
    shapes = (
        (depth, width), (depth, width), (width, depth), None, (taps, width), (taps, width),
        (width,), (width,), (depth,), (depth,), (width,), (2, taps),
    )
    return pl.pallas_call(
        weight_kernel,
        out_shape=tuple(
            jax.ShapeDtypeStruct(grad_in.shape, BF16) if shape is None
            else jax.ShapeDtypeStruct(shape, F32)
            for shape in shapes
        ),
        in_specs=[pl.BlockSpec(memory_space=pltpu.VMEM)] * len(operands),
        out_specs=(pl.BlockSpec(memory_space=pltpu.HBM),) * len(shapes),
        scratch_shapes=[
            pltpu.VMEM((SLOTS, ROWS, width), F32),
            pltpu.VMEM((2, taps, width), F32), pltpu.VMEM((2, taps), F32),
            pltpu.VMEM((width,), F32), pltpu.VMEM((width,), F32), pltpu.VMEM((width,), F32),
            pltpu.VMEM((depth,), F32), pltpu.VMEM((depth,), F32),
            pltpu.SemaphoreType.DMA((SLOTS,)), pltpu.SemaphoreType.DMA((10,)),
        ],
        compiler_params=pltpu.CompilerParams(vmem_limit_bytes=24 * 1024 * 1024),
    )(*operands)


def with_kernels(
    hidden_in, up_act, up_val, cotangent, w_act, w_val, w_down,
    conv_act, conv_val, bias_act, bias_val,
):
    grad_down, all_g, sums, grad_in, norms, down_norms, squares = gradients(
        hidden_in, up_act, up_val, cotangent, w_act, w_val, w_down,
        conv_act, conv_val, bias_act, bias_val,
    )
    (
        grad_w_act, grad_w_val, grad_w_down, grad_input, conv_a, conv_v, bias_a, bias_v,
        rows_a, rows_v, rows_d, conv_rows,
    ) = weight_gradients(
        hidden_in, all_g, grad_down, sums, grad_in, norms, down_norms, squares
    )
    return (
        grad_input, grad_w_act, grad_w_val, grad_w_down, conv_a, conv_v,
        bias_a, bias_v, rows_a, rows_v, rows_d, conv_rows,
    )


def passed_along(value, axis, by):
    length = lax.axis_size(axis)
    pairs = [(i, i + by) for i in range(length) if 0 <= i + by < length]
    return lax.ppermute(value, axis, pairs)


def contract_last(left, right):
    return lax.dot_general(
        left, right, (((1,), (1,)), ((), ())), preferred_element_type=jnp.float32
    )


def contract_first(left, right):
    return lax.dot_general(
        left, right, (((0,), (0,)), ((), ())), preferred_element_type=jnp.float32
    )


def conv_ahead(extended, taps, bias, length):
    total = jnp.zeros((length, extended.shape[1]), jnp.float32) + bias.astype(jnp.float32)
    for offset in range(taps.shape[0]):
        total = total + taps[offset].astype(jnp.float32) * extended[offset : offset + length]
    return total


def conv_behind(extended, taps, length):
    reach = taps.shape[0] - 1
    total = jnp.zeros((length, extended.shape[1]), jnp.float32)
    for offset in range(taps.shape[0]):
        total = (
            total
            + taps[offset].astype(jnp.float32) * extended[reach - offset : reach - offset + length]
        )
    return total.astype(jnp.bfloat16)


def tap_grads(grad_pre, extended, tap_count):
    length = grad_pre.shape[0]
    rows = [
        jnp.sum(grad_pre * extended[offset : offset + length], axis=0)
        for offset in range(tap_count)
    ]
    return (jnp.stack(rows, 0), jnp.sum(grad_pre, axis=0))


def per_device(
    hidden_in,
    up_act,
    up_val,
    cotangent,
    w_act,
    w_val,
    w_down,
    conv_act,
    conv_val,
    bias_act,
    bias_val,
):
    if kernels_fit(up_act, w_down, conv_act):
        return with_kernels(
            hidden_in, up_act, up_val, cotangent, w_act, w_val, w_down,
            conv_act, conv_val, bias_act, bias_val,
        )
    local_rows = cotangent.shape[0]
    tap_count = conv_act.shape[0]
    reach = tap_count - 1
    tp_count = lax.axis_size("tp")
    fs_count = lax.axis_size("fs")
    down_whole = lax.all_gather(w_down, "tp", axis=1, tiled=True)
    prev_act, prev_val = passed_along(
        (up_act[local_rows - reach :], up_val[local_rows - reach :]), "tp", 1
    )
    ext_act = jnp.concatenate([prev_act, up_act], 0).astype(jnp.float32)
    ext_val = jnp.concatenate([prev_val, up_val], 0).astype(jnp.float32)
    pre_act = conv_ahead(ext_act, conv_act, bias_act, local_rows)
    pre_val = conv_ahead(ext_val, conv_val, bias_val, local_rows)
    gelu_act, gelu_back = jax.vjp(jax.nn.gelu, pre_act)
    mixed = (gelu_act * pre_val).astype(jnp.bfloat16)
    grad_mixed = contract_last(cotangent, down_whole).astype(jnp.bfloat16)
    grad_mixed = lax.optimization_barrier(grad_mixed).astype(jnp.float32)
    grad_pre_act = gelu_back(grad_mixed * pre_val)[0]
    grad_pre_val = grad_mixed * gelu_act
    next_act, next_val = passed_along((grad_pre_act[:reach], grad_pre_val[:reach]), "tp", -1)
    grad_up_act = conv_behind(jnp.concatenate([grad_pre_act, next_act], 0), conv_act, local_rows)
    grad_up_val = conv_behind(jnp.concatenate([grad_pre_val, next_val], 0), conv_val, local_rows)
    taps_act, sums_act = tap_grads(grad_pre_act, ext_act, tap_count)
    taps_val, sums_val = tap_grads(grad_pre_val, ext_val, tap_count)
    all_up_act, all_up_val, all_mixed = (
        lax.all_gather(grad_up_act, "tp", axis=0, tiled=True),
        lax.all_gather(grad_up_val, "tp", axis=0, tiled=True),
        lax.all_gather(mixed, "tp", axis=0, tiled=True),
    )
    cot_columns = lax.all_to_all(cotangent, "tp", split_axis=1, concat_axis=0, tiled=True)
    grad_w_act = contract_first(hidden_in, all_up_act)
    grad_w_val = contract_first(hidden_in, all_up_val)
    grad_w_down = contract_first(all_mixed, cot_columns)
    shard_rows = local_rows // fs_count
    block_rows = tp_count * shard_rows

    def select_rows(gathered):
        shaped = gathered.reshape(tp_count, fs_count, shard_rows, gathered.shape[1])
        return jnp.transpose(shaped, (1, 0, 2, 3)).reshape(
            lax.axis_size("fs") * block_rows, gathered.shape[1]
        )

    summed = lax.psum_scatter(
        contract_last(select_rows(all_up_act), w_act)
        + contract_last(select_rows(all_up_val), w_val),
        "fs",
        scatter_dimension=0,
        tiled=True,
    ).astype(jnp.bfloat16)
    grad_input = lax.all_to_all(summed, "tp", split_axis=0, concat_axis=1, tiled=True)
    down_squares = jnp.sum(grad_w_down * grad_w_down, axis=1)
    taps_act, taps_val, sums_act, sums_val, rows_down = lax.psum(
        (taps_act, taps_val, sums_act, sums_val, down_squares), "tp"
    )
    tap_squares = jnp.stack(
        [jnp.sum(taps_act * taps_act, axis=1), jnp.sum(taps_val * taps_val, axis=1)], 0
    )
    rows_act, rows_val, conv_rows = lax.psum(
        (
            jnp.sum(grad_w_act * grad_w_act, axis=1),
            jnp.sum(grad_w_val * grad_w_val, axis=1),
            tap_squares,
        ),
        "fs",
    )
    return (
        grad_input,
        grad_w_act,
        grad_w_val,
        grad_w_down,
        taps_act,
        taps_val,
        sums_act,
        sums_val,
        rows_act,
        rows_val,
        rows_down,
        conv_rows,
    )


def solution(mesh):
    return jax.shard_map(
        per_device,
        mesh=mesh,
        in_specs=(
            P(None, "tp"),
            P("tp", "fs"),
            P("tp", "fs"),
            P("tp", None),
            P("tp", "fs"),
            P("tp", "fs"),
            P("fs", "tp"),
            P(None, "fs"),
            P(None, "fs"),
            P("fs"),
            P("fs"),
        ),
        out_specs=(
            P(("tp", "fs"), None),
            P("tp", "fs"),
            P("tp", "fs"),
            P("fs", "tp"),
            P(None, "fs"),
            P(None, "fs"),
            P("fs"),
            P("fs"),
            P("tp"),
            P("tp"),
            P("fs"),
            P(),
        ),
        check_vma=False,
    )
```
